32 devices in a mesh: rep: 1, fs: 16 (over z, y, x), tp: 2 (over core).
Axes of the slice: x: 2, y: 2, z: 4, core: 2. Of those that a mesh axis runs over, the one named last changes fastest.
Arguments:
- sequence: bfloat16 [16, 768, 2048], P(('rep', 'fs'), None, 'tp'), may hold values from -6 to 6
- mix_gain: float32 [2048], replicated, may hold values from 0.1 to 1.9
- ffn_gain: float32 [2048], replicated, may hold values from 0.1 to 1.9
- proj_outer: float32 [2048, 2048], P(None, ('tp', 'fs')), may hold values from -0.125 to 0.125
- proj_inner: float32 [2048, 2048], P(None, ('tp', 'fs')), may hold values from -0.125 to 0.125
- proj_value: float32 [2048, 2048], P(None, ('tp', 'fs')), may hold values from -0.125 to 0.125
- proj_scales: float32 [3, 2048], P(None, 'tp'), may hold values from 0.5 to 2
- taps: float32 [3, 2048], P(None, 'tp'), may hold values from -3 to 3
- mix_out: float32 [2048, 2048], P('tp', 'fs'), may hold values from -0.125 to 0.125
- mix_out_scale: float32 [2048], P('fs'), may hold values from 0.5 to 2
- ffn_gate: float32 [2048, 2816], P(None, ('tp', 'fs')), may hold values from -0.125 to 0.125
- ffn_up: float32 [2048, 2816], P(None, ('tp', 'fs')), may hold values from -0.125 to 0.125
- ffn_scales: float32 [2, 2816], P(None, 'tp'), may hold values from 0.5 to 2
- ffn_down: float32 [2816, 2048], P('tp', 'fs'), may hold values from -0.109375 to 0.109375
- down_scale: float32 [2048], P('fs'), may hold values from 0.5 to 2
Outputs:
- layer_out: bfloat16 [16, 768, 2048], P(('rep', 'fs'), None, 'tp')
The draws below stay inside these ranges and needn't reach their ends.
All inputs are finite; a program needn't handle non-finite values.
Results may differ from the reference program's by a relative error of at most 0.013.
Values may be sent and summed in bfloat16 or wider, within the bound.
A program may use at most 128 MiB of HBM per device.

```python
import math
import jax
import jax.numpy as jnp
from jax import lax

D = 2048
FF = 2816
LENGTH = 768
SEQS = 16
N_TP = 2


def steps_of(own_key, extent, split, low, largest):
    level = 1.0
    for position, blocks in split:
        draws = jax.random.uniform(jax.random.fold_in(jax.random.fold_in(own_key, 6), position), (blocks,), jnp.float32, low / len(split), largest / len(split))
        level = level * jnp.repeat(jnp.exp(draws), extent[position] // blocks).reshape((-1,) + (1,) * (len(extent) - 1 - position))
    return level


def bell_draw(own_key, extent, scale, bound, shards=(), held_as=jnp.bfloat16):
    result = scale * jax.random.normal(own_key, extent, jnp.float32)
    if shards:
        result = result * steps_of(own_key, extent, shards, -0.22, 0.18)
    return jnp.clip(result, -bound, bound).astype(held_as)


def setup_inputs(seed: int = 0) -> dict:
    keys = jax.random.split(jax.random.key(seed), 16)
    return {
        "sequence": bell_draw(keys[0], (SEQS, LENGTH, D), 1.0, 6.0, ((0, 16), (2, 2))),
        "mix_gain": jnp.clip(1.0 + 0.18 * jax.random.normal(keys[1], (D,), jnp.float32), 0.1, 1.9),
        "ffn_gain": jnp.clip(1.0 + 0.18 * jax.random.normal(keys[2], (D,), jnp.float32), 0.1, 1.9),
        "proj_outer": bell_draw(keys[3], (D, D), D ** -0.5, 0.125, ((1, 32),), jnp.float32),
        "proj_inner": bell_draw(keys[4], (D, D), D ** -0.5, 0.125, ((1, 32),), jnp.float32),
        "proj_value": bell_draw(keys[5], (D, D), D ** -0.5, 0.125, ((1, 32),), jnp.float32),
        "proj_scales": jnp.clip(jnp.exp(math.log(2.0) - 1.3862944 * jax.random.uniform(keys[6], (3, D), jnp.float32) ** steps_of(keys[6], (3, D), ((1, 2),), -0.2, 0.2)), 0.5, 2.0),
        "taps": bell_draw(keys[7], (3, D), 0.6, 3.0, ((1, 2),), jnp.float32),
        "mix_out": bell_draw(keys[8], (D, D), D ** -0.5, 0.125, ((0, 2), (1, 16)), jnp.float32),
        "mix_out_scale": jnp.clip(jnp.exp(math.log(2.0) - 1.3862944 * jax.random.uniform(keys[9], (D,), jnp.float32) ** steps_of(keys[9], (D,), ((0, 16),), -0.2, 0.2)), 0.5, 2.0),
        "ffn_gate": bell_draw(keys[10], (D, FF), D ** -0.5, 0.125, ((1, 32),), jnp.float32),
        "ffn_up": bell_draw(keys[11], (D, FF), D ** -0.5, 0.125, ((1, 32),), jnp.float32),
        "ffn_scales": jnp.clip(jnp.exp(math.log(2.0) - 1.3862944 * jax.random.uniform(keys[12], (2, FF), jnp.float32) ** steps_of(keys[12], (2, FF), ((1, 2),), -0.2, 0.2)), 0.5, 2.0),
        "ffn_down": bell_draw(keys[13], (FF, D), FF ** -0.5, 0.109375, ((0, 2), (1, 16)), jnp.float32),
        "down_scale": jnp.clip(jnp.exp(math.log(2.0) - 1.3862944 * jax.random.uniform(keys[14], (D,), jnp.float32) ** steps_of(keys[14], (D,), ((0, 16),), -0.2, 0.2)), 0.5, 2.0),
    }


eps = 1e-06

def rms_rows(rows, gain):
    values = rows.astype(jnp.float32)
    scaled = values * lax.rsqrt(lax.optimization_barrier(jnp.mean(values * values, axis=-1, keepdims=True)) + eps)
    return (scaled * gain).astype(jnp.bfloat16)

def split_sum(inputs, weight, scale):
    block = inputs.shape[1] // N_TP
    total = jnp.zeros((inputs.shape[0], weight.shape[1]), jnp.float32)
    for index in range(N_TP):
        part = jnp.dot(inputs[:, index * block:(index + 1) * block], weight[index * block:(index + 1) * block], preferred_element_type=jnp.float32) * scale
        rounded = lax.optimization_barrier(part.astype(jnp.bfloat16))
        total = total + rounded.astype(jnp.float32)
    return total

def reference(sequence, mix_gain, ffn_gain, proj_outer, proj_inner, proj_value, proj_scales, taps, mix_out, mix_out_scale, ffn_gate, ffn_up, ffn_scales, ffn_down, down_scale):
    w_outer = proj_outer.astype(jnp.bfloat16)
    w_inner = proj_inner.astype(jnp.bfloat16)
    w_value = proj_value.astype(jnp.bfloat16)
    w_mixout = mix_out.astype(jnp.bfloat16)
    w_gate = ffn_gate.astype(jnp.bfloat16)
    w_up = ffn_up.astype(jnp.bfloat16)
    w_down = ffn_down.astype(jnp.bfloat16)

    def layer(rows):
        normed = rms_rows(rows, mix_gain)
        outer = jnp.dot(normed, w_outer, preferred_element_type=jnp.float32) * proj_scales[0]
        inner = jnp.dot(normed, w_inner, preferred_element_type=jnp.float32) * proj_scales[1]
        value = jnp.dot(normed, w_value, preferred_element_type=jnp.float32) * proj_scales[2]
        carried = inner * value
        length = carried.shape[0]
        back_one = jnp.pad(carried, ((1, 0), (0, 0)))[:length]
        back_two = jnp.pad(carried, ((2, 0), (0, 0)))[:length]
        conv = taps[0] * back_two + taps[1] * back_one + taps[2] * carried
        gated = (outer * conv).astype(jnp.bfloat16)
        mix = split_sum(gated, w_mixout, mix_out_scale)
        after = (rows.astype(jnp.float32) + mix).astype(jnp.bfloat16)
        normed2 = rms_rows(after, ffn_gain)
        gate = jnp.dot(normed2, w_gate, preferred_element_type=jnp.float32) * ffn_scales[0]
        up = jnp.dot(normed2, w_up, preferred_element_type=jnp.float32) * ffn_scales[1]
        hidden = (jax.nn.silu(gate) * up).astype(jnp.bfloat16)
        ffn = split_sum(hidden, w_down, down_scale)
        return (after.astype(jnp.float32) + ffn).astype(jnp.bfloat16)
    return lax.map(layer, sequence)
```

```python
import functools
import math

import jax
import jax.numpy as jnp
from jax import lax
from jax.experimental import pallas as pl
from jax.experimental.pallas import tpu as pltpu
from jax.sharding import PartitionSpec as P

eps = 1e-06
MESH = pl.DeviceIdType.MESH
BF16 = jnp.bfloat16
F32 = jnp.float32
Z, Y, X = 0, 1, 2
ROWS = 256


def grid_of(n):
    side = 2 ** round(math.log2(n) / 3) if n > 1 else 1
    if n % (side * side):
        side = 1
    return (n // (side * side), side, side)


def routes(dims, order):
    found = []
    frontier = [((0, 0, 0), None, 0, 0)]
    while frontier:
        offset, last, way, depth = frontier.pop(0)
        for place, axis in enumerate(order):
            down = 0 if dims[axis] == 2 else dims[axis] - 1
            for step, limit in ((1, dims[axis] - 1), (-1, down)):
                if last is not None and place < last:
                    continue
                if last == place and step != way:
                    continue
                if abs(offset[axis] + step) > limit:
                    continue
                child = list(offset)
                child[axis] += step
                child = tuple(child)
                found.append((child, offset, axis, step, depth + 1))
                frontier.append((child, place, step, depth + 1))
    return found


def product(rows, columns):
    return lax.dot_general(
        rows, columns, (((1,), (1,)), ((), ())), preferred_element_type=F32
    )


def layer_kernel(
    dims,
    seq,
    p_in,
    m_in,
    g_in,
    d_in,
    chan,
    gains,
    hid,
    out,
    pbuf,
    mbuf,
    gbuf,
    dbuf,
    both,
    nbuf,
    gated,
    ext,
    hbuf,
    dsend,
    drecv,
    xsend,
    xrecv,
    frecv,
    w_send,
    w_recv,
    own_sem,
    s_send,
    s_recv,
    x_send,
    x_recv,
    c_send,
    c_recv,
):
    me = lax.axis_index("fs")
    core = lax.axis_index("tp")
    peer = {"tp": 1 - core}
    xp = lax.rem(me, 2)
    partner = {"fs": me + 1 - 2 * xp}
    group = me // 2
    place = (
        group // (dims[1] * dims[2]),
        lax.rem(group // dims[2], dims[1]),
        lax.rem(group, dims[2]),
    )
    members = dims[0] * dims[1] * dims[2]
    length, width = seq.shape
    chunks = length // ROWS
    kch = p_in.shape[2]
    fch = g_in.shape[1]
    cols = m_in.shape[1] - 16
    pair = 2 * cols
    wide = kch * members
    hidden = fch * members
    origin = (0, 0, 0)

    def index(offset):
        at = [lax.rem(place[k] + offset[k] + dims[k], dims[k]) for k in range(3)]
        return (at[0] * dims[1] + at[1]) * dims[2] + at[2]

    def slot_of(offset):
        at = [offset[k] % dims[k] for k in range(3)]
        return (at[0] * dims[1] + at[1]) * dims[2] + at[2]

    def shifted(axis, step):
        return 2 * index(tuple(step if k == axis else 0 for k in range(3))) + xp

    def within(pairs):
        holds = None
        for axis, step in sorted(set(pairs)):
            if dims[axis] == 2 or step == 0:
                continue
            at = place[axis] + step
            one = (at >= 0) if step < 0 else (at < dims[axis])
            holds = one if holds is None else jnp.logical_and(holds, one)
        return holds

    def guarded(holds, act):
        if holds is None:
            act()
        else:
            pl.when(holds)(act)

    def of(step, size):
        return pl.ds(pl.multiple_of(step * size, size), size)

    cut = pair * 2 // 3 // 16 * 16
    views = [
        lambda i: pbuf.at[0, :, of(i, kch)],
        lambda i: pbuf.at[1, :, of(i, kch)],
        lambda i: mbuf.at[i],
        lambda i: gbuf.at[0, of(i, fch)],
        lambda i: gbuf.at[1, of(i, fch)],
        lambda i: dbuf.at[i, pl.ds(0, cut)],
        lambda i: dbuf.at[i, pl.ds(cut, pair - cut)],
    ]
    inputs = {0: p_in.at[0], 1: p_in.at[1], 3: g_in.at[0], 4: g_in.at[1]}
    orders = [(Z, X, Y), (Z, X, Y), (Y, X, Z), (Z, X, Y), (Z, X, Y), (Z, X, Y), (Y, X, Z)]
    plans = [routes(dims, order) for order in orders]
    base = [sum(len(p) for p in plans[:k]) for k in range(len(plans))]
    arrived = [set() for _ in plans]
    sent = []

    def copy_of(part, number):
        child, parent, axis, step, _ = plans[part][number]
        home = views[part](index(parent))
        return pltpu.make_async_remote_copy(
            src_ref=inputs[part] if parent == origin and part in inputs else home,
            dst_ref=home,
            send_sem=w_send.at[base[part] + number],
            recv_sem=w_recv.at[part, slot_of(child)],
            device_id={"fs": shifted(axis, -step)},
            device_id_type=MESH,
        )

    def launch(part, parent):
        for number, item in enumerate(plans[part]):
            if item[1] == parent:
                holds = within(list(enumerate(parent)) + [(item[2], -item[3])])
                guarded(holds, copy_of(part, number).start)
                sent.append((part, number, holds))

    def arrive(part, child):
        if child in arrived[part]:
            return
        arrived[part].add(child)
        block = views[part](index(child))
        ahead = [k for k in range(3) if dims[k] > 1][0]
        there = pltpu.make_async_remote_copy(
            src_ref=block,
            dst_ref=block,
            send_sem=w_send.at[0],
            recv_sem=w_recv.at[part, slot_of(child)],
            device_id={"fs": shifted(ahead, 1)},
            device_id_type=MESH,
        )
        guarded(within(list(enumerate(child))), there.wait_recv)

    def parents(part, depth):
        found = []
        for child, parent, axis, step, level in plans[part]:
            if level == depth + 1 and parent not in found:
                found.append(parent)
        return found

    def relay(part, depth):
        for parent in parents(part, depth):
            arrive(part, parent)
            launch(part, parent)

    def finish(part):
        for item in plans[part]:
            arrive(part, item[0])

    deepest = [max(item[4] for item in p) for p in plans]

    near = [(axis, 1) for axis in range(3) if dims[axis] > 1]
    near += [(axis, -1) for axis in range(3) if dims[axis] > 2]
    barrier = pltpu.get_barrier_semaphore()
    for axis, step in near:
        pl.semaphore_signal(
            barrier, inc=1, device_id={"fs": shifted(axis, step)}, device_id_type=MESH
        )
    pl.semaphore_signal(barrier, inc=1, device_id=partner, device_id_type=MESH)
    pl.semaphore_signal(barrier, inc=1, device_id=peer, device_id_type=MESH)
    pl.semaphore_wait(barrier, len(near) + 2)

    def to(where, src, dst, send, recv):
        return pltpu.make_async_remote_copy(
            src_ref=src,
            dst_ref=dst,
            send_sem=send,
            recv_sem=recv,
            device_id=where,
            device_id_type=MESH,
        )

    mine = of(core, width)
    theirs = of(1 - core, width)

    def rows(r):
        return of(r, ROWS)

    seq_local = pltpu.make_async_copy(seq, both.at[0, :, mine], own_sem.at[0])
    seq_peer = to(peer, seq, both.at[0, :, mine], s_send.at[0], s_recv.at[0])
    seq_partner = [
        to(
            partner,
            seq.at[pl.ds(r * ROWS, ROWS)],
            both.at[1, pl.ds(r * ROWS, ROWS), mine],
            s_send.at[1 + r],
            s_recv.at[1 + r],
        )
        for r in range(chunks)
    ]
    seq_pass = [
        to(
            peer,
            both.at[1, pl.ds(r * ROWS, ROWS), mine],
            both.at[1, pl.ds(r * ROWS, ROWS), mine],
            s_send.at[1 + chunks + r],
            s_recv.at[1 + chunks + r],
        )
        for r in range(chunks)
    ]
    cross = []
    locals_ = [seq_local]
    side = of(xp, cols)
    tail = pl.ds(pl.multiple_of(pair + xp * 16, 16), 16)
    for k, (src, dst) in enumerate(
        (
            (lambda t: m_in.at[t, pl.ds(0, cols)], mbuf.at[group, side]),
            (lambda t: m_in.at[t, pl.ds(cols, 16)], mbuf.at[group, tail]),
            (lambda t: d_in.at[t], dbuf.at[group, side]),
        )
    ):
        at = 1 + 2 * chunks + k
        cross.append(to(partner, src(1 - xp), dst, s_send.at[at], s_recv.at[at]))
        locals_.append(pltpu.make_async_copy(src(xp), dst, own_sem.at[1 + k]))
    for k, part in enumerate(sorted(inputs)):
        locals_.append(
            pltpu.make_async_copy(inputs[part], views[part](group), own_sem.at[4 + k])
        )

    launch(0, origin)
    for copy in seq_partner:
        copy.start()
    seq_peer.start()
    for copy in locals_:
        copy.start()
    for copy in cross:
        copy.start()
    launch(1, origin)

    def norm(s, first, count, gain):
        tall = 16

        def step(i, _):
            at = pl.ds(pl.multiple_of(first + i * tall, tall), tall)
            values = both[s, at, :].astype(F32)
            mean = jnp.mean(values * values, axis=-1, keepdims=True)
            scaled = values * lax.rsqrt(mean + eps)
            nbuf[s, at, :] = (scaled * gains[pl.ds(gain, 1), :]).astype(BF16)
            return 0

        lax.fori_loop(0, count // tall, step, 0)

    def project(k, s):
        ext[0:8, :] = jnp.zeros((8, wide), F32)

        def step(r, _):
            block = nbuf[s, rows(r), :]
            inner = product(block, pbuf[k, 1]) * chan[k, 1:2, :]
            value = product(block, pbuf[k, 2]) * chan[k, 2:3, :]
            carried = inner * value
            ext[8 : 8 + ROWS, :] = carried
            conv = chan[k, 3:4, :] * ext[6 : 6 + ROWS, :]
            conv = conv + chan[k, 4:5, :] * ext[7 : 7 + ROWS, :]
            conv = conv + chan[k, 5:6, :] * carried
            ext[0:8, :] = ext[ROWS : ROWS + 8, :]
            outer = product(block, pbuf[k, 0]) * chan[k, 0:1, :]
            gated[s, rows(r), pl.ds(k * wide, wide)] = (outer * conv).astype(BF16)
            return 0

        lax.fori_loop(0, chunks, step, 0)

    def exchange(kind, s, r):
        at = kind * 2 * chunks + s * chunks + r
        home = drecv.at[s, rows(r)]
        return to(peer, dsend.at[s, rows(r)], home, c_send.at[at], c_recv.at[at])

    def spread(s, r):
        at = 4 * chunks + s * chunks + r
        home = both.at[s, rows(r), mine]
        return to(peer, home, home, c_send.at[at], c_recv.at[at])

    def crossing(s, r):
        return to(
            partner,
            xsend.at[s, rows(r)],
            xrecv.at[1 - s, rows(r)],
            x_send.at[s * chunks + r],
            x_recv.at[(1 - s) * chunks + r],
        )

    def crossed(s, r):
        return to(
            partner,
            xsend.at[s, rows(r)],
            xrecv.at[s, rows(r)],
            x_send.at[s * chunks + r],
            x_recv.at[s * chunks + r],
        )

    def last(r):
        at = 2 * chunks + r
        return to(
            partner, xsend.at[1, rows(r)], frecv.at[rows(r)], x_send.at[at], x_recv.at[at]
        )

    half = members // 2

    def scale_of(g, which):
        scale = jnp.zeros((1, pair), F32)
        for side_ in range(2):
            tile = mbuf[g, pl.ds(pair + 16 * side_, 16), pl.ds(0, pair)].astype(F32)
            for k in range(3):
                scale = scale + tile[3 * which + k : 3 * which + k + 1]
        return scale

    def partial(rows_value, buf, which, s, r):
        def away(i, _):
            g = (1 - core) * half + i
            term = product(rows_value(), buf[g, pl.ds(0, pair), :]) * scale_of(g, which)
            dsend[s, rows(r), of(i, pair)] = term.astype(BF16)
            return 0

        def keep(i, _):
            g = core * half + i
            term = product(rows_value(), buf[g, pl.ds(0, pair), :]) * scale_of(g, which)
            xsend[s, rows(r), of(i, pair)] = term.astype(BF16)
            return 0

        lax.fori_loop(0, half, away, 0)
        exchange(which, s, r).start()
        lax.fori_loop(0, half, keep, 0)

    def each(act):
        def step(r, _):
            act(r)
            return 0

        lax.fori_loop(0, chunks, step, 0)

    def mix_terms(s):
        each(lambda r: partial(lambda: gated[s, rows(r), :], mbuf, 0, s, r))

    def add_peer(which, s, r):
        copy = exchange(which, s, r)
        copy.wait_recv()
        total = xsend[s, rows(r), :].astype(F32) + drecv[s, rows(r), :].astype(F32)
        xsend[s, rows(r), :] = total.astype(BF16)
        copy.wait_send()

    def mix_cross(s):
        def act(r):
            add_peer(0, s, r)
            crossing(s, r).start()

        each(act)

    def mix_after(s):
        def act(r):
            crossed(s, r).wait_recv()
            mix = xsend[s, rows(r), :].astype(F32) + xrecv[s, rows(r), :].astype(F32)
            after = both[s, rows(r), mine].astype(F32) + mix
            both[s, rows(r), mine] = after.astype(BF16)
            spread(s, r).start()
            crossing(s, r).wait_send()

        each(act)

    def feed(s):
        def act(r):
            spread(s, r).wait_recv()
            norm(s, r * ROWS, ROWS, 1)
            block = nbuf.at[s, rows(r)]

            def unit(i, _):
                at = of(i, wide)
                gate = product(block[...], gbuf[0, at, :]) * hid[0:1, at]
                up = product(block[...], gbuf[1, at, :]) * hid[1:2, at]
                hbuf[:, at] = (gate / (1.0 + jnp.exp(-gate)) * up).astype(BF16)
                return 0

            lax.fori_loop(0, hidden // wide, unit, 0)
            partial(lambda: hbuf[...], dbuf, 1, s, r)

        each(act)

    def feed_cross():
        def act(r):
            add_peer(1, 1, r)
            last(r).start()

        each(act)

    def close():
        def act(r):
            copy = exchange(1, 0, r)
            copy.wait_recv()
            last(r).wait_recv()
            ffn = xsend[0, rows(r), :].astype(F32) + drecv[0, rows(r), :].astype(F32)
            ffn = ffn + frecv[rows(r), :].astype(F32)
            after = both[0, rows(r), mine].astype(F32)
            out[rows(r), :] = (after + ffn).astype(BF16)
            copy.wait_send()

        each(act)

    seq_local.wait()
    seq_peer.wait_recv()
    norm(0, 0, length, 0)
    for depth in range(1, deepest[0]):
        relay(0, depth)
        if depth <= chunks:
            seq_partner[depth - 1].wait_recv()
            seq_pass[depth - 1].start()
    for r in range(deepest[0] - 1, chunks):
        seq_partner[r].wait_recv()
        seq_pass[r].start()
    for copy in locals_[1:4]:
        copy.wait()
    for copy in cross:
        copy.wait_recv()
    launch(2, origin)
    relay(1, 1)
    finish(0)
    for copy in locals_[4:]:
        copy.wait()
    project(0, 0)
    relay(1, 2)
    for copy in seq_pass:
        copy.wait()
    norm(1, 0, length, 0)
    launch(3, origin)
    for depth in range(3, deepest[1]):
        relay(1, depth)
    relay(2, 1)
    project(0, 1)
    for depth in range(2, deepest[2]):
        relay(2, depth)
    finish(1)
    project(1, 1)
    relay(3, 1)
    launch(4, origin)
    project(1, 0)
    relay(3, 2)
    finish(2)
    mix_terms(1)
    mix_cross(1)
    for depth in range(3, deepest[3]):
        relay(3, depth)
    relay(4, 1)
    mix_terms(0)
    mix_cross(0)
    launch(6, origin)
    launch(5, origin)
    relay(4, 2)
    for depth in range(1, deepest[6]):
        relay(6, depth)
    for depth in range(3, deepest[4]):
        relay(4, depth)
    relay(5, 1)
    mix_after(1)
    for depth in range(2, deepest[5]):
        relay(5, depth)
    finish(3)
    finish(4)
    finish(5)
    finish(6)
    feed(1)
    mix_after(0)
    feed_cross()
    feed(0)
    close()
    for part, number, holds in sent:
        guarded(holds, copy_of(part, number).wait_send)
    seq_peer.wait_send()
    for copy in seq_partner + cross:
        copy.wait_send()
    for s in range(2):
        each(lambda r: spread(s, r).wait_send())
    each(lambda r: last(r).wait_send())


def prepare(
    n,
    proj_outer,
    proj_inner,
    proj_value,
    proj_scales,
    taps,
    mix_out,
    mix_out_scale,
    ffn_gate,
    ffn_up,
    ffn_scales,
    ffn_down,
    down_scale,
):
    half = n // 2
    xp = lax.rem(lax.axis_index("fs"), 2)
    each = proj_outer.shape[1]
    kch = each // 2
    p_in = jnp.stack(
        [w.astype(BF16).T.reshape(2, kch, -1) for w in (proj_outer, proj_inner, proj_value)],
        axis=1,
    )
    units = ffn_gate.shape[1]
    fill = -units % 16
    g_in = jnp.stack(
        [jnp.pad(w.astype(BF16).T, ((0, fill), (0, 0))) for w in (ffn_gate, ffn_up)]
    )
    cols = mix_out.shape[1]
    mixed = mix_out.astype(BF16).T.reshape(cols, half, 2, 2, kch)
    mixed = mixed.transpose(2, 0, 3, 1, 4).reshape(2, cols, half * each)
    thin = []
    for scale in (mix_out_scale, down_scale):
        high = lax.reduce_precision(scale, 8, 7)
        middle = lax.reduce_precision(scale - high, 8, 7)
        thin += [high, middle, scale - high - middle]
    thin = jnp.stack(thin)
    ours = (lax.iota(jnp.int32, 2 * cols) // cols == xp)[None]
    thin = jnp.where(ours, jnp.concatenate([thin, thin], 1), 0.0).astype(BF16)
    thin = jnp.pad(thin, ((0, 10), (0, half * each - 2 * cols)))
    m_in = jnp.concatenate([mixed, jnp.broadcast_to(thin, (2,) + thin.shape)], axis=1)
    down = ffn_down.astype(BF16).T.reshape(cols, half, 2, units)
    d_in = jnp.pad(down, ((0, 0), (0, 0), (0, 0), (0, fill))).transpose(2, 0, 1, 3)
    d_in = d_in.reshape(2, cols, -1)
    chan = jnp.concatenate([proj_scales, taps]).reshape(6, half, 2, 2, kch)
    chan = lax.dynamic_index_in_dim(chan, xp, 2, keepdims=False)
    chan = chan.transpose(2, 0, 1, 3).reshape(2, 6, half * kch)
    chan = jnp.pad(chan, ((0, 0), (0, 2), (0, 0)))
    hid = ffn_scales.reshape(2, half, 2, units)
    hid = lax.dynamic_index_in_dim(hid, xp, 2, keepdims=False)
    hid = jnp.pad(hid, ((0, 6), (0, 0), (0, fill))).reshape(8, -1)
    return p_in, m_in, g_in, d_in, chan, hid


def body(n, sequence, mix_gain, ffn_gain, *rest):
    seq = sequence[0]
    length, width = seq.shape
    depth = 2 * width
    p_in, m_in, g_in, d_in, chan, hid = prepare(n, *rest)
    gains = jnp.pad(jnp.stack([mix_gain, ffn_gain]), ((0, 6), (0, 0)))
    full = grid_of(n)
    dims = (full[0], full[1], full[2] // 2)
    members = n // 2
    kch, fch = p_in.shape[2], g_in.shape[1]
    cols = m_in.shape[1] - 16
    chunks = length // ROWS
    items = 7 * len(routes(dims, (Z, X, Y))) + 2 * members * 7
    operands = (seq, p_in, m_in, g_in, d_in, chan, gains, hid)
    result = pl.pallas_call(
        functools.partial(layer_kernel, dims),
        out_shape=jax.ShapeDtypeStruct(seq.shape, BF16),
        in_specs=[pl.BlockSpec(memory_space=pltpu.VMEM)] * len(operands),
        out_specs=pl.BlockSpec(memory_space=pltpu.VMEM),
        scratch_shapes=[
            pltpu.VMEM((2, 3, members * kch, depth), BF16),
            pltpu.VMEM((members, 2 * cols + 32, m_in.shape[2]), BF16),
            pltpu.VMEM((2, members * fch, depth), BF16),
            pltpu.VMEM((members, 2 * cols, d_in.shape[2]), BF16),
            pltpu.VMEM((2, length, depth), BF16),
            pltpu.VMEM((2, length, depth), BF16),
            pltpu.VMEM((2, length, m_in.shape[2]), BF16),
            pltpu.VMEM((8 + ROWS, members * kch), F32),
            pltpu.VMEM((ROWS, members * fch), BF16),
            pltpu.VMEM((2, length, width), BF16),
            pltpu.VMEM((2, length, width), BF16),
            pltpu.VMEM((2, length, width), BF16),
            pltpu.VMEM((2, length, width), BF16),
            pltpu.VMEM((length, width), BF16),
            pltpu.SemaphoreType.DMA((items,)),
            pltpu.SemaphoreType.DMA((7, members)),
            pltpu.SemaphoreType.DMA((8,)),
            pltpu.SemaphoreType.DMA((4 + 2 * chunks,)),
            pltpu.SemaphoreType.DMA((4 + 2 * chunks,)),
            pltpu.SemaphoreType.DMA((3 * chunks,)),
            pltpu.SemaphoreType.DMA((3 * chunks,)),
            pltpu.SemaphoreType.DMA((6 * chunks,)),
            pltpu.SemaphoreType.DMA((6 * chunks,)),
        ],
        compiler_params=pltpu.CompilerParams(
            collective_id=0, has_side_effects=True, vmem_limit_bytes=67043328
        ),
        name="layer",
    )(*operands)
    return result[None]


def solution(mesh):
    in_specs = (
        P(("rep", "fs"), None, "tp"),
        P(),
        P(),
        P(None, ("tp", "fs")),
        P(None, ("tp", "fs")),
        P(None, ("tp", "fs")),
        P(None, "tp"),
        P(None, "tp"),
        P("tp", "fs"),
        P("fs"),
        P(None, ("tp", "fs")),
        P(None, ("tp", "fs")),
        P(None, "tp"),
        P("tp", "fs"),
        P("fs"),
    )
    out_specs = P(("rep", "fs"), None, "tp")
    return jax.shard_map(
        functools.partial(body, mesh.shape["fs"]),
        mesh=mesh,
        in_specs=in_specs,
        out_specs=out_specs,
        check_vma=False,
    )
```

```python
import functools
import math

import jax
import jax.numpy as jnp
from jax import lax
from jax.experimental import pallas as pl
from jax.experimental.pallas import tpu as pltpu
from jax.sharding import PartitionSpec as P

eps = 1e-06
MESH = pl.DeviceIdType.MESH
BF16 = jnp.bfloat16
F32 = jnp.float32
Z, Y, X = 0, 1, 2
ROWS = 256


def grid_of(n):
    side = 2 ** round(math.log2(n) / 3) if n > 1 else 1
    if n % (side * side):
        side = 1
    return (n // (side * side), side, side)


def routes(dims, order):
    found = []
    frontier = [((0, 0, 0), None, 0, 0)]
    while frontier:
        offset, last, way, depth = frontier.pop(0)
        for place, axis in enumerate(order):
            down = 0 if dims[axis] == 2 else dims[axis] - 1
            for step, limit in ((1, dims[axis] - 1), (-1, down)):
                if last is not None and place < last:
                    continue
                if last == place and step != way:
                    continue
                if abs(offset[axis] + step) > limit:
                    continue
                child = list(offset)
                child[axis] += step
                child = tuple(child)
                found.append((child, offset, axis, step, depth + 1))
                frontier.append((child, place, step, depth + 1))
    return found


def product(rows, columns):
    return lax.dot_general(
        rows, columns, (((1,), (1,)), ((), ())), preferred_element_type=F32
    )


def scoped(act):
    def run(*given):
        numbers = [str(g) for g in given if isinstance(g, int)]
        with jax.named_scope("_".join([act.__name__] + numbers)):
            return act(*given)

    return run


class Group:
    def __init__(self, full, halved, place):
        self.full, self.halved = full, halved
        self.dims = tuple(d // 2 if k == halved else d for k, d in enumerate(full))
        self.place = tuple(p // 2 if k == halved else p for k, p in enumerate(place))
        self.parity = lax.rem(place[halved], 2)
        self.size = self.dims[0] * self.dims[1] * self.dims[2]

    def at(self, offset):
        return [
            lax.rem(self.place[k] + offset[k] + self.dims[k], self.dims[k]) for k in range(3)
        ]

    def index(self, offset):
        at = self.at(offset)
        return (at[0] * self.dims[1] + at[1]) * self.dims[2] + at[2]

    def device(self, offset):
        at = self.at(offset)
        at[self.halved] = 2 * at[self.halved] + self.parity
        return (at[0] * self.full[1] + at[1]) * self.full[2] + at[2]

    def neighbour(self, axis, step):
        return self.device(tuple(step if k == axis else 0 for k in range(3)))

    def slot(self, offset):
        at = [offset[k] % self.dims[k] for k in range(3)]
        return (at[0] * self.dims[1] + at[1]) * self.dims[2] + at[2]

    def within(self, pairs):
        holds = None
        for axis, step in sorted(set(pairs)):
            if self.dims[axis] == 2 or step == 0:
                continue
            at = self.place[axis] + step
            one = (at >= 0) if step < 0 else (at < self.dims[axis])
            holds = one if holds is None else jnp.logical_and(holds, one)
        return holds

    def near(self):
        found = [(axis, 1) for axis in range(3) if self.dims[axis] > 1]
        return found + [(axis, -1) for axis in range(3) if self.dims[axis] > 2]


def guarded(holds, act):
    if holds is None:
        act()
    else:
        pl.when(holds)(act)


def of(step, size):
    if isinstance(step, int):
        return pl.ds(step * size, size)
    return pl.ds(pl.multiple_of(step * size, size), size)


def rows(r):
    return of(r, ROWS)


def to(where, src, dst, send, recv):
    return pltpu.make_async_remote_copy(
        src_ref=src,
        dst_ref=dst,
        send_sem=send,
        recv_sem=recv,
        device_id=where,
        device_id_type=MESH,
    )


ORDERS = [
    (0, (Z, X, Y)),
    (0, (Z, X, Y)),
    (0, (Z, X, Y)),
    (0, (Z, X, Y)),
    (1, (Z, Y, X)),
    (1, (Z, Y, X)),
    (1, (Z, Y, X)),
    (1, (Z, Y, X)),
]
ORDER = ";".join(
    [
        "launch 0 1",
        "launch 1 0",
        "launch 0 0",
        "d_cross",
        "launch 1 1",
        "m_cross",
        "m_wait",
        "launch 2 1",
        "launch 3 0",
        "launch 3 1",
        "seq",
        "relay 0 1",
        "launch 5 2",
        "relay 3 1",
        "relay 1 1",
        "relay 3 2",
        "launch 5 0",
        "launch 4 2",
        "norm 0",
        "pass_seq 0",
        "pass_seq 1",
        "relay 3 3",
        "pass_seq 2",
        "d_wait",
        "relay 1 2",
        "relay 1 3",
        "seq_wait",
        "launch 2 0",
        "relay 5 1",
        "relay 5 2",
        "finish 3",
        "launch 6 2",
        "relay 0 2",
        "launch 7 2",
        "launch 4 0",
        "relay 0 3",
        "finish 1",
        "project 1 0",
        "relay 5 3",
        "relay 2 1",
        "relay 4 1",
        "relay 2 2",
        "norm 1",
        "finish 0",
        "project 0 1",
        "relay 4 2",
        "relay 2 3",
        "finish 2",
        "launch 7 0",
        "launch 6 0",
        "project 1 1",
        "relay 4 3",
        "scales",
        "project 0 0",
        "mix_terms 1",
        "finish 5",
        "mix_cross",
        "relay 6 1",
        "mix_terms 0",
        "mix_after 0",
        "mix_after 1",
        "relay 7 1",
        "relay 7 2",
        "relay 7 3",
        "finish 4",
        "relay 6 2",
        "feed 0 0",
        "pass_on 0",
        "feed 0 1",
        "feed 1 0",
        "mix_after 2",
        "feed 0 2",
        "pass_on 1",
        "E 0",
        "feed 1 1",
        "pass_on 2",
        "relay 6 3",
        "E 1",
        "feed 1 2",
        "E 2",
        "L 0",
        "L 1",
        "L 2",
        "Z 0",
        "Z 1",
        "end",
    ]
)


def layer_kernel(
    full,
    seq,
    p_in,
    m_in,
    g_in,
    d_in,
    chan,
    gains,
    hid,
    out,
    pbuf,
    mbuf,
    gbuf,
    dbuf,
    both,
    aft,
    nbuf,
    gated,
    ext,
    hbuf,
    sbuf,
    dsend,
    drecv,
    xsend,
    xrecv,
    frecv,
    w_send,
    w_recv,
    own_sem,
    s_send,
    s_recv,
    x_send,
    x_recv,
    c_send,
    c_recv,
    d_send,
    d_recv,
    y_send,
    y_recv,
):
    me = lax.axis_index("fs")
    core = lax.axis_index("tp")
    peer = {"tp": 1 - core}
    here = (me // (full[1] * full[2]), lax.rem(me // full[2], full[1]), lax.rem(me, full[2]))
    mixer, feeder = Group(full, X, here), Group(full, Y, here)
    groups = (mixer, feeder)
    xp, yp = mixer.parity, feeder.parity
    beside = {"fs": me + 1 - 2 * xp}
    across = {"fs": me + (1 - 2 * yp) * full[2]}
    members = mixer.size
    length, width = seq.shape
    chunks = length // ROWS
    kch = p_in.shape[2]
    fch = g_in.shape[1]
    cols = m_in.shape[1] - 16
    pair = 2 * cols
    span = full[2] * cols
    wide = kch * members
    hidden = fch * members
    origin = (0, 0, 0)
    cut = (pair + 32) // 2 // 16 * 16
    views = [
        lambda i: pbuf.at[0, :, of(i, kch)],
        lambda i: pbuf.at[1, :, of(i, kch)],
        lambda i: mbuf.at[i, pl.ds(0, cut)],
        lambda i: mbuf.at[i, pl.ds(cut, pair + 32 - cut)],
        lambda i: gbuf.at[0, of(i, fch)],
        lambda i: gbuf.at[1, of(i, fch)],
        lambda i: dbuf.at[0, of(i, cols)],
        lambda i: dbuf.at[1, of(i, cols)],
    ]
    inputs = {0: p_in.at[0], 1: p_in.at[1], 4: g_in.at[0], 5: g_in.at[1]}
    plans = [routes(groups[g].dims, order) for g, order in ORDERS]
    base = [sum(len(p) for p in plans[:k]) for k in range(len(plans))]
    deepest = [max(item[4] for item in p) for p in plans]
    arrived = [set() for _ in plans]
    sent = []

    def copy_of(part, number):
        group = groups[ORDERS[part][0]]
        child, parent, axis, step, _ = plans[part][number]
        home = views[part](group.index(parent))
        return to(
            {"fs": group.neighbour(axis, -step)},
            inputs[part] if parent == origin and part in inputs else home,
            home,
            w_send.at[base[part] + number],
            w_recv.at[part, group.slot(child)],
        )

    def launch(part, only=None, parent=origin):
        group = groups[ORDERS[part][0]]
        for number, item in enumerate(plans[part]):
            if item[1] == parent and only in (None, item[2]):
                holds = group.within(list(enumerate(parent)) + [(item[2], -item[3])])
                guarded(holds, copy_of(part, number).start)
                sent.append((part, number, holds))

    def arrive(part, child):
        if child in arrived[part] or child == origin:
            return
        arrived[part].add(child)
        group = groups[ORDERS[part][0]]
        block = views[part](group.index(child))
        there = to(
            peer, block, block, w_send.at[0], w_recv.at[part, group.slot(child)]
        )
        guarded(group.within(list(enumerate(child))), there.wait_recv)

    @scoped
    def relay(part, depth):
        for number, item in enumerate(plans[part]):
            parent = item[1]
            if item[4] == depth + 1 and all(p[1] != parent for p in plans[part][:number]):
                arrive(part, parent)
                launch(part, None, parent)

    @scoped
    def finish(part):
        for item in plans[part]:
            arrive(part, item[0])

    barrier = pltpu.get_barrier_semaphore()
    greeted = [{"fs": g.neighbour(*hop)} for g in groups for hop in g.near()]
    greeted += [beside, across, peer]
    for device in greeted:
        pl.semaphore_signal(barrier, inc=1, device_id=device, device_id_type=MESH)
    pl.semaphore_wait(barrier, len(greeted))

    mine = of(core, width)

    seq_local = pltpu.make_async_copy(seq, both.at[0, :, mine], own_sem.at[0])
    seq_peer = to(peer, seq, both.at[0, :, mine], s_send.at[0], s_recv.at[0])
    seq_beside, seq_pass = [], []
    for r in range(chunks):
        home = both.at[1, rows(r), mine]
        seq_beside.append(
            to(beside, seq.at[rows(r)], home, s_send.at[1 + r], s_recv.at[1 + r])
        )
        at = 1 + chunks + r
        seq_pass.append(to(peer, home, home, s_send.at[at], s_recv.at[at]))
    side = of(xp, cols)
    ends = pl.ds(pl.multiple_of(pair + xp * 16, 16), 16)
    at = 1 + 2 * chunks
    m_home = mbuf.at[mixer.index(origin), side]
    e_home = mbuf.at[mixer.index(origin), ends]
    d_home = dbuf.at[yp, of(feeder.index(origin), cols)]
    body_, end_ = pl.ds(0, cols), pl.ds(cols, 16)
    m_cross = [
        to(beside, m_in.at[1 - xp, body_], m_home, s_send.at[at], s_recv.at[at]),
        to(beside, m_in.at[1 - xp, end_], e_home, s_send.at[at + 1], s_recv.at[at + 1]),
    ]
    d_cross = to(across, d_in.at[1 - yp], d_home, s_send.at[at + 2], s_recv.at[at + 2])
    d_there = dbuf.at[1 - yp, of(feeder.index(origin), cols)]
    d_landed = to(across, d_there, d_there, s_send.at[at + 2], s_recv.at[at + 2])
    m_there = [
        mbuf.at[mixer.index(origin), of(1 - xp, cols)],
        mbuf.at[
            mixer.index(origin), pl.ds(pl.multiple_of(pair + (1 - xp) * 16, 16), 16)
        ],
    ]
    m_landed = [
        to(beside, ref, ref, s_send.at[at + k], s_recv.at[at + k])
        for k, ref in enumerate(m_there)
    ]
    own = [
        pltpu.make_async_copy(m_in.at[xp, body_], m_home, own_sem.at[1]),
        pltpu.make_async_copy(m_in.at[xp, end_], e_home, own_sem.at[2]),
        pltpu.make_async_copy(d_in.at[yp], d_home, own_sem.at[3]),
    ]
    for k, part in enumerate(sorted(inputs)):
        home = views[part](groups[ORDERS[part][0]].index(origin))
        own.append(pltpu.make_async_copy(inputs[part], home, own_sem.at[4 + k]))

    @scoped
    def norm(source, target, first, count, gain):
        tall, deep = 16, 4

        def step(i, _):
            spots = [
                pl.ds(pl.multiple_of(first + (i * deep + k) * tall, tall), tall)
                for k in range(deep)
            ]
            factors = []
            for spot in spots:
                values = source[spot, :].astype(F32)
                mean = jnp.mean(values * values, axis=-1, keepdims=True)
                factors.append(lax.rsqrt(mean + eps))
            for spot, factor in zip(spots, factors):
                scaled = source[spot, :].astype(F32) * factor
                nbuf[target, spot, :] = (scaled * gains[pl.ds(gain, 1), :]).astype(BF16)
            return 0

        lax.fori_loop(0, count // (tall * deep), step, 0)

    def each(act):
        def step(r, _):
            act(r)
            return 0

        lax.fori_loop(0, chunks, step, 0)

    @scoped
    def project(k, s):
        ext[0:8, :] = jnp.zeros((8, wide), F32)

        def act(r):
            block = nbuf[s, rows(r), :]
            inner = product(block, pbuf[k, 1]) * chan[k, 1:2, :]
            value = product(block, pbuf[k, 2]) * chan[k, 2:3, :]
            carried = inner * value
            ext[8 : 8 + ROWS, :] = carried
            conv = chan[k, 3:4, :] * ext[6 : 6 + ROWS, :]
            conv = conv + chan[k, 4:5, :] * ext[7 : 7 + ROWS, :]
            conv = conv + chan[k, 5:6, :] * carried
            ext[0:8, :] = ext[ROWS : ROWS + 8, :]
            outer = product(block, pbuf[k, 0]) * chan[k, 0:1, :]
            gated[s, rows(r), pl.ds(k * wide, wide)] = (outer * conv).astype(BF16)

        each(act)

    @scoped
    def scales():
        def step(g, _):
            tiles = [
                mbuf[g, pl.ds(pair + 16 * e, 16), pl.ds(0, pair)].astype(F32)
                for e in range(2)
            ]
            for which in range(2):
                scale = jnp.zeros((1, pair), F32)
                for tile in tiles:
                    for k in range(3):
                        scale = scale + tile[3 * which + k : 3 * which + k + 1]
                sbuf[which : which + 1, of(g, pair)] = scale
            return 0

        lax.fori_loop(0, members, step, 0)

    def exchange(s, r):
        at = s * chunks + r
        home = drecv.at[s, rows(r)]
        return to(peer, dsend.at[s, rows(r)], home, c_send.at[at], c_recv.at[at])

    def crossing(r):
        return to(beside, xsend.at[1, rows(r)], xrecv.at[rows(r)], x_send.at[r], x_recv.at[r])

    def spread(r):
        at = 2 * chunks + r
        home = both.at[0, rows(r), mine]
        return to(peer, home, home, c_send.at[at], c_recv.at[at])

    def afar(r):
        at = chunks + r
        return to(
            across, both.at[0, rows(r), mine], aft.at[rows(r), mine], x_send.at[at], x_recv.at[at]
        )

    def onward(r):
        at = 3 * chunks + r
        home = aft.at[rows(r), mine]
        return to(peer, home, home, c_send.at[at], c_recv.at[at])

    half = members // 2

    @scoped
    def mix_terms(s):
        def act(r):
            def away(i, _):
                g = (1 - core) * half + i
                term = product(gated[s, rows(r), :], mbuf[g, pl.ds(0, pair), :])
                dsend[s, rows(r), of(i, pair)] = (term * sbuf[0:1, of(g, pair)]).astype(BF16)
                return 0

            def keep(i, _):
                g = core * half + i
                term = product(gated[s, rows(r), :], mbuf[g, pl.ds(0, pair), :])
                xsend[s, rows(r), of(i, pair)] = (term * sbuf[0:1, of(g, pair)]).astype(BF16)
                return 0

            for i in range(half):
                away(i, 0)
            exchange(s, r).start()
            for i in range(half):
                keep(i, 0)

        each(act)

    @scoped
    def mix_cross():
        def act(r):
            copy = exchange(1, r)
            copy.wait_recv()
            total = xsend[1, rows(r), :].astype(F32) + drecv[1, rows(r), :].astype(F32)
            xsend[1, rows(r), :] = total.astype(BF16)
            crossing(r).start()

        each(act)

    @scoped
    def mix_after(r):
        exchange(0, r).wait_recv()
        crossing(r).wait_recv()
        mix = xsend[0, rows(r), :].astype(F32) + drecv[0, rows(r), :].astype(F32)
        mix = mix + xrecv[rows(r), :].astype(F32)
        after = both[0, rows(r), mine].astype(F32) + mix
        both[0, rows(r), mine] = after.astype(BF16)
        afar(r).start()
        spread(r).start()

    @scoped
    def pass_on(r):
        afar(r).wait_recv()
        onward(r).start()

    @scoped
    def feed(s, r):
        (spread, onward)[s](r).wait_recv()
        norm((both.at[0], aft)[s], s, r * ROWS, ROWS, 1)

        def unit(i, _):
            at = of(i, wide)
            block = nbuf[s, rows(r), :]
            gate = product(block, gbuf[0, at, :]) * hid[0:1, at]
            up = product(block, gbuf[1, at, :]) * hid[1:2, at]
            hbuf[s, rows(r), at] = (gate / (1.0 + jnp.exp(-gate)) * up).astype(BF16)
            return 0

        lax.fori_loop(0, hidden // wide, unit, 0)

    blocks = 2 * feeder.dims[0] * feeder.dims[1]
    held = blocks // 2

    def where(j, spot):
        at = feeder.at(spot)
        return (at[0] * feeder.dims[1] + at[1]) * 2 + j

    def inside(spot, holds=None):
        there = feeder.within(list(enumerate(spot)))
        if there is None or holds is None:
            return holds if there is None else there
        return jnp.logical_and(holds, there)

    def lent(s, b, r):
        at = (s * blocks + b) * chunks + r
        local = of(lax.rem(b, held), span)
        return to(
            peer,
            nbuf.at[s, rows(r), of(b, span)],
            drecv.at[s, rows(r), local],
            d_send.at[at],
            d_recv.at[at],
        )

    def sends(b, r):
        at = b * chunks + r
        local = of(lax.rem(b, held), span)
        return to(
            across,
            nbuf.at[1, rows(r), of(b, span)],
            frecv.at[rows(r), local],
            y_send.at[at],
            y_recv.at[at],
        )

    spots = sorted(
        {(item[0][0], item[0][1], 0) for item in plans[6]} | {origin},
        key=lambda o: (abs(o[0]) + abs(o[1]), o),
    )
    units = [
        [(j, spot) for spot in spots for j in range(2) if (abs(spot[0]) + abs(spot[1]) < 2) == near]
        for near in (True, False)
    ]

    def landed(j, spot):
        for item in plans[6 + j]:
            if item[0][:2] == spot[:2]:
                arrive(6 + j, item[0])

    def term(s, j, spot, r):
        b = where(j, spot)
        value = product(hbuf[s, rows(r), :], dbuf[j, of(b // 2, span), :])
        value = value * sbuf[1:2, of(b, span)]
        nbuf[s, rows(r), of(b, span)] = value.astype(BF16)
        pl.when(b // held != core)(lent(s, b, r).start)

    def settle(j, spot, r):
        b = where(j, spot)

        def run():
            lent(1, b, r).wait_recv()
            theirs = drecv[1, rows(r), of(lax.rem(b, held), span)]
            total = nbuf[1, rows(r), of(b, span)].astype(F32) + theirs.astype(F32)
            nbuf[1, rows(r), of(b, span)] = total.astype(BF16)
            sends(b, r).start()

        pl.when(inside(spot, b // held == core))(run)

    @scoped
    def down(late, r):
        ahead = None
        for j, spot in units[late]:
            landed(j, spot)
            guarded(inside(spot), functools.partial(term, 1, j, spot, r))
            if ahead:
                settle(*ahead, r)
            ahead = (j, spot)
        if ahead:
            settle(*ahead, r)

    @scoped
    def down_own(late):
        for j, spot in units[late]:
            landed(j, spot)
            guarded(inside(spot), lambda: each(functools.partial(term, 0, j, spot)))

    def close(j, spot):
        b = where(j, spot)
        local = of(lax.rem(b, held), span)

        def act(r):
            lent(0, b, r).wait_recv()
            sends(b, r).wait_recv()
            ffn = nbuf[0, rows(r), of(b, span)].astype(F32)
            ffn = ffn + drecv[0, rows(r), local].astype(F32)
            ffn = ffn + frecv[rows(r), local].astype(F32)
            after = both[0, rows(r), of(b, span)].astype(F32)
            out[rows(r), local] = (after + ffn).astype(BF16)

        pl.when(inside(spot, b // held == core))(lambda: each(act))

    @scoped
    def end():
        for j, spot in units[0] + units[1]:
            close(j, spot)

    @scoped
    def seq_start():
        for copy in seq_beside:
            copy.start()

    @scoped
    def m_cross_start():
        for copy in m_cross:
            copy.start()

    @scoped
    def m_wait():
        for copy in own[:2]:
            copy.wait()
        for copy in m_landed:
            copy.wait_recv()

    @scoped
    def d_wait():
        own[2].wait()
        d_landed.wait_recv()

    @scoped
    def pass_seq(r):
        seq_beside[r].wait_recv()
        seq_pass[r].start()

    @scoped
    def seq_wait():
        for copy in seq_pass:
            copy.wait()

    def norm_of(s):
        if s == 0:
            seq_local.wait()
            seq_peer.wait_recv()
        norm(both.at[s], s, 0, length, 0)

    def finished(part):
        finish(part)
        if part in inputs:
            own[3 + sorted(inputs).index(part)].wait()

    def relays(part, depth):
        if depth < deepest[part]:
            relay(part, depth)

    acts = {
        "launch": launch,
        "relay": relays,
        "finish": finished,
        "seq": seq_start,
        "m_cross": m_cross_start,
        "m_wait": m_wait,
        "d_cross": lambda: d_cross.start(),
        "d_wait": d_wait,
        "pass_seq": pass_seq,
        "seq_wait": seq_wait,
        "norm": norm_of,
        "project": project,
        "scales": scales,
        "mix_terms": mix_terms,
        "mix_cross": mix_cross,
        "mix_after": mix_after,
        "pass_on": pass_on,
        "feed": feed,
        "E": functools.partial(down, 0),
        "L": functools.partial(down, 1),
        "Z": down_own,
        "end": end,
    }
    seq_peer.start()
    seq_local.start()
    for copy in own:
        copy.start()
    extra = max(deepest) - 1
    for line in ORDER.split(";"):
        name, *given = line.split()
        given = [int(g) for g in given]
        acts[name](*given)
        if name == "relay" and given[1] == 3:
            for depth in range(4, extra + 1):
                relays(given[0], depth)
    for part, number, holds in sent:
        guarded(holds, copy_of(part, number).wait_send)
    seq_peer.wait_send()
    d_cross.wait_send()
    for copy in seq_beside + m_cross:
        copy.wait_send()

    def drain(r):
        crossing(r).wait_send()
        for s in range(2):
            exchange(s, r).wait_send()
        spread(r).wait_send()
        afar(r).wait_send()
        onward(r).wait_send()
        for k in range(held):
            sends(core * held + k, r).wait_send()
            for s in range(2):
                lent(s, (1 - core) * held + k, r).wait_send()

    each(drain)


def prepare(
    full,
    proj_outer,
    proj_inner,
    proj_value,
    proj_scales,
    taps,
    mix_out,
    mix_out_scale,
    ffn_gate,
    ffn_up,
    ffn_scales,
    ffn_down,
    down_scale,
):
    half = full[0] * full[1] * full[2] // 2
    lines, columns = half // full[2], full[2]
    me = lax.axis_index("fs")
    xp, yp = lax.rem(me, 2), lax.rem(me // columns, 2)
    each = proj_outer.shape[1]
    kch = each // 2
    p_in = jnp.stack(
        [w.astype(BF16).T.reshape(2, kch, -1) for w in (proj_outer, proj_inner, proj_value)],
        axis=1,
    )
    units = ffn_gate.shape[1]
    fill = -units % 16
    g_in = jnp.stack(
        [jnp.pad(w.astype(BF16).T, ((0, fill), (0, 0))) for w in (ffn_gate, ffn_up)]
    )
    cols = mix_out.shape[1]
    mixed = mix_out.astype(BF16).T.reshape(cols, half, 2, 2, kch)
    mixed = mixed.transpose(2, 0, 3, 1, 4).reshape(2, cols, half * each)
    thin = []
    for scale in (mix_out_scale, down_scale):
        high = lax.reduce_precision(scale, 8, 7)
        middle = lax.reduce_precision(scale - high, 8, 7)
        thin += [high, middle, scale - high - middle]
    thin = jnp.stack(thin)
    ours = (lax.iota(jnp.int32, 2 * cols) // cols == xp)[None]
    thin = jnp.where(ours, jnp.concatenate([thin, thin], 1), 0.0).astype(BF16)
    thin = jnp.pad(thin, ((0, 10), (0, half * each - 2 * cols)))
    m_in = jnp.concatenate([mixed, jnp.broadcast_to(thin, (2,) + thin.shape)], axis=1)
    down = ffn_down.astype(BF16).T.reshape(cols, lines, 2, columns, units)
    down = jnp.pad(down, ((0, 0), (0, 0), (0, 0), (0, 0), (0, fill)))
    d_in = down.transpose(2, 0, 1, 3, 4).reshape(2, cols, -1)
    chan = jnp.concatenate([proj_scales, taps]).reshape(6, half, 2, 2, kch)
    chan = lax.dynamic_index_in_dim(chan, xp, 2, keepdims=False)
    chan = chan.transpose(2, 0, 1, 3).reshape(2, 6, half * kch)
    chan = jnp.pad(chan, ((0, 0), (0, 2), (0, 0)))
    hid = ffn_scales.reshape(2, lines, 2, columns, units)
    hid = lax.dynamic_index_in_dim(hid, yp, 2, keepdims=False)
    hid = jnp.pad(hid, ((0, 6), (0, 0), (0, 0), (0, fill))).reshape(8, -1)
    return p_in, m_in, g_in, d_in, chan, hid


def body(n, sequence, mix_gain, ffn_gain, *rest):
    seq = sequence[0]
    length, width = seq.shape
    depth = 2 * width
    full = grid_of(n)
    p_in, m_in, g_in, d_in, chan, hid = prepare(full, *rest)
    gains = jnp.pad(jnp.stack([mix_gain, ffn_gain]), ((0, 6), (0, 0)))
    members = n // 2
    kch, fch = p_in.shape[2], g_in.shape[1]
    cols = m_in.shape[1] - 16
    chunks = length // ROWS
    units = members * fch
    items = len(ORDERS) * 4 * members
    operands = (seq, p_in, m_in, g_in, d_in, chan, gains, hid)
    sems = [pltpu.SemaphoreType.DMA((k,)) for k in (items,)]
    sems += [pltpu.SemaphoreType.DMA((len(ORDERS), members)), pltpu.SemaphoreType.DMA((8,))]
    for k in (4 + 2 * chunks, 2 * chunks, 4 * chunks, 2 * n * chunks, n * chunks):
        sems += [pltpu.SemaphoreType.DMA((k,))] * 2
    result = pl.pallas_call(
        functools.partial(layer_kernel, full),
        out_shape=jax.ShapeDtypeStruct(seq.shape, BF16),
        in_specs=[pl.BlockSpec(memory_space=pltpu.VMEM)] * len(operands),
        out_specs=pl.BlockSpec(memory_space=pltpu.VMEM),
        scratch_shapes=[
            pltpu.VMEM((2, 3, members * kch, depth), BF16),
            pltpu.VMEM((members, 2 * cols + 32, m_in.shape[2]), BF16),
            pltpu.VMEM((2, units, depth), BF16),
            pltpu.VMEM((2, members * cols, units), BF16),
            pltpu.VMEM((2, length, depth), BF16),
            pltpu.VMEM((length, depth), BF16),
            pltpu.VMEM((2, length, depth), BF16),
            pltpu.VMEM((2, length, m_in.shape[2]), BF16),
            pltpu.VMEM((8 + ROWS, members * kch), F32),
            pltpu.VMEM((2, length, units), BF16),
            pltpu.VMEM((8, depth), F32),
            pltpu.VMEM((2, length, width), BF16),
            pltpu.VMEM((2, length, width), BF16),
            pltpu.VMEM((2, length, width), BF16),
            pltpu.VMEM((length, width), BF16),
            pltpu.VMEM((length, width), BF16),
        ]
        + sems,
        compiler_params=pltpu.CompilerParams(
            collective_id=0, has_side_effects=True, vmem_limit_bytes=67043328
        ),
        name="layer",
    )(*operands)
    return result[None]


def solution(mesh):
    in_specs = (
        P(("rep", "fs"), None, "tp"),
        P(),
        P(),
        P(None, ("tp", "fs")),
        P(None, ("tp", "fs")),
        P(None, ("tp", "fs")),
        P(None, "tp"),
        P(None, "tp"),
        P("tp", "fs"),
        P("fs"),
        P(None, ("tp", "fs")),
        P(None, ("tp", "fs")),
        P(None, "tp"),
        P("tp", "fs"),
        P("fs"),
    )
    out_specs = P(("rep", "fs"), None, "tp")
    return jax.shard_map(
        functools.partial(body, mesh.shape["fs"]),
        mesh=mesh,
        in_specs=in_specs,
        out_specs=out_specs,
        check_vma=False,
    )
```

```python
import functools
import math

import jax
import jax.numpy as jnp
from jax import lax
from jax.experimental import pallas as pl
from jax.experimental.pallas import tpu as pltpu
from jax.sharding import PartitionSpec as P

eps = 1e-06
MESH = pl.DeviceIdType.MESH
BF16 = jnp.bfloat16
F32 = jnp.float32
Z, Y, X = 0, 1, 2
ROWS = 256


def grid_of(n):
    side = 2 ** round(math.log2(n) / 3) if n > 1 else 1
    if n % (side * side):
        side = 1
    return (n // (side * side), side, side)


def routes(dims, order):
    found = []
    frontier = [((0, 0, 0), None, 0, 0)]
    while frontier:
        offset, last, way, depth = frontier.pop(0)
        for place, axis in enumerate(order):
            down = 0 if dims[axis] == 2 else dims[axis] - 1
            for step, limit in ((1, dims[axis] - 1), (-1, down)):
                if last is not None and place < last:
                    continue
                if last == place and step != way:
                    continue
                if abs(offset[axis] + step) > limit:
                    continue
                child = list(offset)
                child[axis] += step
                child = tuple(child)
                found.append((child, offset, axis, step, depth + 1))
                frontier.append((child, place, step, depth + 1))
    return found


def product(rows, columns):
    return lax.dot_general(
        rows, columns, (((1,), (1,)), ((), ())), preferred_element_type=F32
    )


def scoped(act):
    def run(*given):
        numbers = [str(g) for g in given if isinstance(g, int)]
        with jax.named_scope("_".join([act.__name__] + numbers)):
            return act(*given)

    return run


class Group:
    def __init__(self, full, halved, place):
        self.full, self.halved = full, halved
        self.dims = tuple(d // 2 if k == halved else d for k, d in enumerate(full))
        self.place = tuple(p // 2 if k == halved else p for k, p in enumerate(place))
        self.parity = lax.rem(place[halved], 2)
        self.size = self.dims[0] * self.dims[1] * self.dims[2]

    def at(self, offset):
        return [
            lax.rem(self.place[k] + offset[k] + self.dims[k], self.dims[k]) for k in range(3)
        ]

    def index(self, offset):
        at = self.at(offset)
        return (at[0] * self.dims[1] + at[1]) * self.dims[2] + at[2]

    def device(self, offset):
        at = self.at(offset)
        at[self.halved] = 2 * at[self.halved] + self.parity
        return (at[0] * self.full[1] + at[1]) * self.full[2] + at[2]

    def neighbour(self, axis, step):
        return self.device(tuple(step if k == axis else 0 for k in range(3)))

    def slot(self, offset):
        at = [offset[k] % self.dims[k] for k in range(3)]
        return (at[0] * self.dims[1] + at[1]) * self.dims[2] + at[2]

    def within(self, pairs):
        holds = None
        for axis, step in sorted(set(pairs)):
            if self.dims[axis] == 2 or step == 0:
                continue
            at = self.place[axis] + step
            one = (at >= 0) if step < 0 else (at < self.dims[axis])
            holds = one if holds is None else jnp.logical_and(holds, one)
        return holds

    def near(self):
        found = [(axis, 1) for axis in range(3) if self.dims[axis] > 1]
        return found + [(axis, -1) for axis in range(3) if self.dims[axis] > 2]


def guarded(holds, act):
    if holds is None:
        act()
    else:
        pl.when(holds)(act)


def of(step, size):
    if isinstance(step, int):
        return pl.ds(step * size, size)
    return pl.ds(pl.multiple_of(step * size, size), size)


def rows(r):
    return of(r, ROWS)


def to(where, src, dst, send, recv):
    return pltpu.make_async_remote_copy(
        src_ref=src,
        dst_ref=dst,
        send_sem=send,
        recv_sem=recv,
        device_id=where,
        device_id_type=MESH,
    )


ORDERS = [
    (0, (Z, X, Y)),
    (0, (Z, X, Y)),
    (0, (Z, X, Y)),
    (0, (Z, X, Y)),
    (1, (Z, Y, X)),
    (1, (Z, Y, X)),
    (1, (X, Y, Z)),
    (1, (X, Y, Z)),
]
(
    LAUNCH, RELAY, FINISH, ROWS_SWAP, MIX_SWAP, MIX_WAIT, DOWN_SWAP, DOWN_WAIT, ROWS_PASS,
    ROWS_WAIT, NORM, PROJECT, SCALES, MIX_AWAY, MIX_OWN, MIX_SEND, MIX_AFTER, AFTER_PASS, FEED_UP,
    FEED_GATE, DOWN_NEAR, DOWN_FAR, DOWN_OWN, END,
) = range(24)

ORDER = (
    (LAUNCH, 1, 0), (LAUNCH, 1, 1), (MIX_SWAP,), (DOWN_SWAP,), (LAUNCH, 5, 2), (NORM, 0), (MIX_WAIT,),
    (LAUNCH, 3, 0), (RELAY, 1, 0), (RELAY, 1, 1), (LAUNCH, 0, 0), (LAUNCH, 4, 2), (RELAY, 1, 3),
    (LAUNCH, 3, 1), (DOWN_WAIT,), (RELAY, 1, 2), (RELAY, 3, 1), (ROWS_SWAP,), (RELAY, 3, 0),
    (RELAY, 1, 4), (RELAY, 3, 2), (RELAY, 3, 4), (LAUNCH, 2, 0), (RELAY, 2, 0), (LAUNCH, 6, 2), (RELAY, 1, 5),
    (RELAY, 3, 3), (RELAY, 3, 5), (LAUNCH, 5, 0), (RELAY, 0, 1), (LAUNCH, 7, 2), (FINISH, 1),
    (PROJECT, 1, 0), (RELAY, 0, 0), (RELAY, 2, 1), (FINISH, 3), (RELAY, 5, 1), (ROWS_PASS, 0),
    (ROWS_PASS, 1), (RELAY, 5, 0), (LAUNCH, 0, 1), (RELAY, 2, 3), (RELAY, 0, 3), (RELAY, 0, 2),
    (LAUNCH, 4, 0), (RELAY, 0, 4), (ROWS_PASS, 2), (RELAY, 2, 5), (ROWS_WAIT,), (RELAY, 2, 2),
    (RELAY, 5, 2), (NORM, 1), (RELAY, 5, 3), (RELAY, 0, 5), (RELAY, 4, 1), (LAUNCH, 2, 1), (PROJECT, 1, 1),
    (RELAY, 5, 5), (RELAY, 2, 4), (RELAY, 4, 0), (FINISH, 0), (PROJECT, 0, 1), (RELAY, 5, 4), (FINISH, 2),
    (SCALES,), (RELAY, 6, 0), (LAUNCH, 6, 0), (MIX_AWAY, 0), (MIX_AWAY, 1), (MIX_AWAY, 2),
    (MIX_SEND, 0), (MIX_SEND, 1), (LAUNCH, 7, 0), (MIX_SEND, 2), (PROJECT, 0, 0), (MIX_OWN, 0),
    (RELAY, 4, 3), (MIX_OWN, 2), (RELAY, 6, 3), (MIX_OWN, 1), (MIX_AFTER, 0), (RELAY, 6, 4),
    (MIX_AFTER, 1), (RELAY, 7, 0), (RELAY, 7, 1), (FINISH, 5), (FEED_UP, 0, 1), (FEED_UP, 0, 0),
    (RELAY, 4, 2), (RELAY, 4, 4), (RELAY, 4, 5), (MIX_AFTER, 2), (RELAY, 7, 3), (RELAY, 6, 1), (RELAY, 7, 4),
    (FEED_UP, 0, 2), (AFTER_PASS, 0), (AFTER_PASS, 1), (RELAY, 7, 2), (FEED_UP, 1, 0), (RELAY, 6, 2),
    (FEED_UP, 1, 1), (RELAY, 7, 7), (FINISH, 4), (FEED_GATE, 1, 0), (RELAY, 6, 8), (AFTER_PASS, 2),
    (RELAY, 7, 5), (RELAY, 7, 6), (DOWN_NEAR, 0), (RELAY, 6, 5), (FEED_GATE, 1, 1), (DOWN_NEAR, 1),
    (RELAY, 7, 8), (FEED_UP, 1, 2), (FEED_GATE, 1, 2), (RELAY, 6, 7), (RELAY, 6, 6), (DOWN_FAR, 0),
    (DOWN_FAR, 1), (FEED_GATE, 0, 0), (FEED_GATE, 0, 1), (DOWN_NEAR, 2), (DOWN_FAR, 2),
    (FEED_GATE, 0, 2), (DOWN_OWN, 0), (DOWN_OWN, 1), (END,),
)


def layer_kernel(
    full,
    seq,
    po_in,
    pi_in,
    pv_in,
    m_in,
    gate_in,
    up_in,
    d_in,
    thin,
    chan,
    mix_gain,
    ffn_gain,
    hid,
    out,
    pbuf,
    mbuf,
    gbuf,
    dbuf,
    both,
    aft,
    nbuf,
    gated,
    ext,
    hbuf,
    sbuf,
    m_out,
    d_out,
    m_tmp,
    d_tmp,
    dsend,
    drecv,
    xsend,
    xrecv,
    frecv,
    w_send,
    w_recv,
    own_sem,
    s_send,
    s_recv,
    x_send,
    x_recv,
    c_send,
    c_recv,
    d_send,
    d_recv,
    y_send,
    y_recv,
):
    me = lax.axis_index("fs")
    core = lax.axis_index("tp")
    peer = {"tp": 1 - core}
    here = (me // (full[1] * full[2]), lax.rem(me // full[2], full[1]), lax.rem(me, full[2]))
    mixer, feeder = Group(full, X, here), Group(full, Y, here)
    groups = (mixer, feeder)
    xp, yp = mixer.parity, feeder.parity
    beside = {"fs": me + 1 - 2 * xp}
    across = {"fs": me + (1 - 2 * yp) * full[2]}
    members = mixer.size
    length, width = seq.shape
    chunks = length // ROWS
    kch = po_in.shape[0] // 2
    units_in = gate_in.shape[0]
    units_sent = units_in + -units_in % 8
    fch = gbuf.shape[1] // members
    cols = m_in.shape[1]
    pair = 2 * cols
    span = full[2] * cols
    wide = kch * members
    hidden = fch * members
    origin = (0, 0, 0)
    cut = (pair + 32) // 2 // 16 * 16
    views = [
        lambda i: pbuf.at[0, :, of(i, kch)],
        lambda i: pbuf.at[1, :, of(i, kch)],
        lambda i: mbuf.at[i, pl.ds(0, cut)],
        lambda i: mbuf.at[i, pl.ds(cut, pair + 32 - cut)],
        lambda i: gbuf.at[0, pl.ds(pl.multiple_of(i * fch, 16), units_sent)],
        lambda i: gbuf.at[1, pl.ds(pl.multiple_of(i * fch, 16), units_sent)],
        lambda i: dbuf.at[0, of(i, cols)],
        lambda i: dbuf.at[1, of(i, cols)],
    ]
    plans = [routes(groups[g].dims, order) for g, order in ORDERS]
    base = [sum(len(p) for p in plans[:k]) for k in range(len(plans))]
    deepest = [max(item[4] for item in p) for p in plans]
    arrived = [set() for _ in plans]
    sent = []

    def copy_of(part, number):
        group = groups[ORDERS[part][0]]
        child, parent, axis, step, _ = plans[part][number]
        home = views[part](group.index(parent))
        return to(
            {"fs": group.neighbour(axis, -step)},
            home,
            home,
            w_send.at[base[part] + number],
            w_recv.at[part, group.slot(child)],
        )

    def launch(part, only=None, parent=origin):
        group = groups[ORDERS[part][0]]
        for number, item in enumerate(plans[part]):
            if item[1] == parent and only in (None, item[2]):
                holds = group.within(list(enumerate(parent)) + [(item[2], -item[3])])
                guarded(holds, copy_of(part, number).start)
                sent.append((part, number, holds))

    def arrive(part, child):
        if child in arrived[part] or child == origin:
            return
        arrived[part].add(child)
        group = groups[ORDERS[part][0]]
        block = views[part](group.index(child))
        there = to(
            peer, block, block, w_send.at[0], w_recv.at[part, group.slot(child)]
        )
        guarded(group.within(list(enumerate(child))), there.wait_recv)

    forks = []
    for plan in plans:
        found = []
        for item in sorted(plan, key=lambda item: item[4]):
            if item[1] != origin and item[1] not in found:
                found.append(item[1])
        forks.append(found)

    @scoped
    def relay(part, number):
        arrive(part, forks[part][number])
        launch(part, None, forks[part][number])

    @scoped
    def finish(part):
        for item in plans[part]:
            arrive(part, item[0])

    if fch > units_in:
        for which in range(2):
            for i in range(members):
                spot = pl.ds(i * fch + units_in, fch - units_in)
                gbuf[which, spot, :] = jnp.zeros((fch - units_in, 2 * width), BF16)

    barrier = pltpu.get_barrier_semaphore()
    greeted = [{"fs": g.neighbour(*hop)} for g in groups for hop in g.near()]
    greeted += [beside, across, peer]
    for device in greeted:
        pl.semaphore_signal(barrier, inc=1, device_id=device, device_id_type=MESH)
    pl.semaphore_wait(barrier, len(greeted))

    mine = of(core, width)

    seq_local = pltpu.make_async_copy(seq, both.at[0, :, mine], own_sem.at[0])
    seq_peer = to(peer, seq, both.at[0, :, mine], s_send.at[0], s_recv.at[0])
    seq_beside, seq_pass = [], []
    for r in range(chunks):
        home = both.at[1, rows(r), mine]
        seq_beside.append(
            to(beside, seq.at[rows(r)], home, s_send.at[1 + r], s_recv.at[1 + r])
        )
        at = 1 + chunks + r
        seq_pass.append(to(peer, home, home, s_send.at[at], s_recv.at[at]))
    side = of(xp, cols)
    ends = pl.ds(pl.multiple_of(pair + xp * 16, 16), 16)
    at = 1 + 2 * chunks
    m_home = mbuf.at[mixer.index(origin), side]
    e_home = mbuf.at[mixer.index(origin), ends]
    d_home = dbuf.at[yp, of(feeder.index(origin), cols)]
    m_cross = [
        to(beside, m_out, m_home, s_send.at[at], s_recv.at[at]),
        to(beside, thin, e_home, s_send.at[at + 1], s_recv.at[at + 1]),
    ]
    d_cross = to(across, d_out, d_home, s_send.at[at + 2], s_recv.at[at + 2])
    d_there = dbuf.at[1 - yp, of(feeder.index(origin), cols)]
    d_landed = to(across, d_there, d_there, s_send.at[at + 2], s_recv.at[at + 2])
    m_there = [
        mbuf.at[mixer.index(origin), of(1 - xp, cols)],
        mbuf.at[
            mixer.index(origin), pl.ds(pl.multiple_of(pair + (1 - xp) * 16, 16), 16)
        ],
    ]
    m_landed = [
        to(beside, ref, ref, s_send.at[at + k], s_recv.at[at + k])
        for k, ref in enumerate(m_there)
    ]

    @scoped
    def p_ready():
        spot = of(mixer.index(origin), kch)
        for k in range(2):
            for which, ref in enumerate((po_in, pi_in, pv_in)):
                pbuf[k, which, spot, :] = ref[pl.ds(k * kch, kch), :].astype(BF16)

    @scoped
    def g_ready():
        spot = pl.ds(pl.multiple_of(feeder.index(origin) * fch, 16), units_in)
        for which, ref in enumerate((gate_in, up_in)):
            gbuf[which, spot, :] = ref[...].astype(BF16)

    @scoped
    def m_ready():
        each_in = 2 * kch
        for target in range(2):
            to_x = xp if target else 1 - xp
            for g in range(members):
                for k in range(2):
                    source = pl.multiple_of((2 * g + to_x) * each_in + k * kch, kch)
                    m_tmp[pl.ds(k * wide + g * kch, kch), :] = m_in[pl.ds(source, kch), :]
            for tile in range(m_tmp.shape[0] // 128):
                at_ = pl.ds(tile * 128, 128)
                turned = m_tmp[at_, :].T.astype(BF16)
                if target:
                    m_home[:, at_] = turned
                else:
                    m_out[:, at_] = turned
        e_home[...] = thin[...]

    @scoped
    def d_ready():
        for target in range(2):
            to_y = yp if target else 1 - yp
            for i in range(members):
                line, x = i // full[2], i % full[2]
                source = ((2 * line + to_y) * full[2] + x) * units_in
                spot = pl.ds(i * fch, units_in)
                d_tmp[spot, :] = d_in[pl.ds(pl.multiple_of(source, 4), units_in), :]
                if fch > units_in:
                    fill = fch - units_in
                    d_tmp[pl.ds(i * fch + units_in, fill), :] = jnp.zeros((fill, cols), F32)
            for tile in range(d_tmp.shape[0] // 128):
                at_ = pl.ds(tile * 128, 128)
                turned = d_tmp[at_, :].T.astype(BF16)
                if target:
                    d_home[:, at_] = turned
                else:
                    d_out[:, at_] = turned

    @scoped
    def norm(source, target, first, count, gains):
        tall, deep = 16, 4

        def step(i, _):
            spots = [
                pl.ds(pl.multiple_of(first + (i * deep + k) * tall, tall), tall)
                for k in range(deep)
            ]
            factors = []
            for spot in spots:
                values = source[spot, :].astype(F32)
                mean = jnp.mean(values * values, axis=-1, keepdims=True)
                factors.append(lax.rsqrt(mean + eps))
            for spot, factor in zip(spots, factors):
                scaled = source[spot, :].astype(F32) * factor
                nbuf[target, spot, :] = (scaled * gains[...]).astype(BF16)
            return 0

        lax.fori_loop(0, count // (tall * deep), step, 0)

    def each(act):
        def step(r, _):
            act(r)
            return 0

        lax.fori_loop(0, chunks, step, 0)

    @scoped
    def project(k, s):
        ext[0:8, :] = jnp.zeros((8, wide), F32)

        def act(r):
            block = nbuf[s, rows(r), :]
            inner = product(block, pbuf[k, 1]) * chan[k, 1:2, :]
            value = product(block, pbuf[k, 2]) * chan[k, 2:3, :]
            carried = inner * value
            ext[8 : 8 + ROWS, :] = carried
            conv = chan[k, 3:4, :] * ext[6 : 6 + ROWS, :]
            conv = conv + chan[k, 4:5, :] * ext[7 : 7 + ROWS, :]
            conv = conv + chan[k, 5:6, :] * carried
            ext[0:8, :] = ext[ROWS : ROWS + 8, :]
            outer = product(block, pbuf[k, 0]) * chan[k, 0:1, :]
            gated[s, rows(r), pl.ds(k * wide, wide)] = (outer * conv).astype(BF16)

        each(act)

    @scoped
    def scales():
        def step(g, _):
            tiles = [
                mbuf[g, pl.ds(pair + 16 * e, 16), pl.ds(0, pair)].astype(F32)
                for e in range(2)
            ]
            for which in range(2):
                scale = jnp.zeros((1, pair), F32)
                for tile in tiles:
                    for k in range(3):
                        scale = scale + tile[3 * which + k : 3 * which + k + 1]
                sbuf[which : which + 1, of(g, pair)] = scale
            return 0

        lax.fori_loop(0, members, step, 0)

    def exchange(s, r):
        at = s * chunks + r
        home = drecv.at[s, rows(r)]
        return to(peer, dsend.at[s, rows(r)], home, c_send.at[at], c_recv.at[at])

    def crossing(r):
        return to(beside, xsend.at[1, rows(r)], xrecv.at[rows(r)], x_send.at[r], x_recv.at[r])

    def spread(r):
        at = 2 * chunks + r
        home = both.at[0, rows(r), mine]
        return to(peer, home, home, c_send.at[at], c_recv.at[at])

    def afar(r):
        at = chunks + r
        return to(
            across, both.at[0, rows(r), mine], aft.at[rows(r), mine], x_send.at[at], x_recv.at[at]
        )

    def onward(r):
        at = 3 * chunks + r
        home = aft.at[rows(r), mine]
        return to(peer, home, home, c_send.at[at], c_recv.at[at])

    half = members // 2

    @scoped
    def mix_terms(s, r):
        def block(g, ref, i):
            term = product(gated[s, rows(r), :], mbuf[g, pl.ds(0, pair), :])
            ref[s, rows(r), of(i, pair)] = (term * sbuf[0:1, of(g, pair)]).astype(BF16)

        for i in range(half):
            block((1 - core) * half + i, dsend, i)
        exchange(s, r).start()
        for i in range(half):
            block(core * half + i, xsend, i)

    @scoped
    def mix_cross(r):
        exchange(1, r).wait_recv()
        total = xsend[1, rows(r), :].astype(F32) + drecv[1, rows(r), :].astype(F32)
        xsend[1, rows(r), :] = total.astype(BF16)
        crossing(r).start()

    @scoped
    def mix_after(r):
        exchange(0, r).wait_recv()
        crossing(r).wait_recv()
        mix = xsend[0, rows(r), :].astype(F32) + drecv[0, rows(r), :].astype(F32)
        mix = mix + xrecv[rows(r), :].astype(F32)
        after = both[0, rows(r), mine].astype(F32) + mix
        both[0, rows(r), mine] = after.astype(BF16)
        afar(r).start()
        spread(r).start()

    @scoped
    def pass_on(r):
        afar(r).wait_recv()
        onward(r).start()

    def wide_steps(act):
        def step(i, _):
            act(of(i, wide))
            return 0

        lax.fori_loop(0, hidden // wide, step, 0)

    @scoped
    def feed_up(s, r):
        (spread, onward)[s](r).wait_recv()
        norm((both.at[0], aft)[s], s, r * ROWS, ROWS, ffn_gain)

        def act(at):
            up = product(nbuf[s, rows(r), :], gbuf[1, at, :]) * hid[1:2, at]
            hbuf[s, rows(r), at] = up.astype(BF16)

        wide_steps(act)

    @scoped
    def feed(s, r):
        def act(at):
            gate = product(nbuf[s, rows(r), :], gbuf[0, at, :]) * hid[0:1, at]
            up = hbuf[s, rows(r), at].astype(F32)
            hbuf[s, rows(r), at] = (gate / (1.0 + jnp.exp(-gate)) * up).astype(BF16)

        wide_steps(act)

    blocks = 2 * feeder.dims[0] * feeder.dims[1]
    held = blocks // 2

    def where(j, spot):
        at = feeder.at(spot)
        return (at[0] * feeder.dims[1] + at[1]) * 2 + j

    def inside(spot, holds=None):
        there = feeder.within(list(enumerate(spot)))
        if there is None or holds is None:
            return holds if there is None else there
        return jnp.logical_and(holds, there)

    def lent(s, b, r):
        at = (s * held + lax.rem(b, held)) * chunks + r
        local = of(lax.rem(b, held), span)
        return to(
            peer,
            nbuf.at[s, rows(r), of(b, span)],
            drecv.at[s, rows(r), local],
            d_send.at[at],
            d_recv.at[at],
        )

    def sends(b, r):
        at = lax.rem(b, held) * chunks + r
        local = of(lax.rem(b, held), span)
        return to(
            across,
            nbuf.at[1, rows(r), of(b, span)],
            frecv.at[rows(r), local],
            y_send.at[at],
            y_recv.at[at],
        )

    spots = sorted(
        {(item[0][0], item[0][1], 0) for item in plans[6]} | {origin},
        key=lambda o: (abs(o[0]) + abs(o[1]), o),
    )
    units = [
        [(j, spot) for spot in spots for j in range(2) if (abs(spot[0]) + abs(spot[1]) < 2) == near]
        for near in (True, False)
    ]

    def landed(j, spot):
        for item in plans[6 + j]:
            if item[0][:2] == spot[:2]:
                arrive(6 + j, item[0])

    def term(s, j, spot, r):
        b = where(j, spot)
        value = product(hbuf[s, rows(r), :], dbuf[j, of(b // 2, span), :])
        value = value * sbuf[1:2, of(b, span)]
        nbuf[s, rows(r), of(b, span)] = value.astype(BF16)
        pl.when(b // held != core)(lent(s, b, r).start)

    def settle(j, spot, r):
        b = where(j, spot)

        def run():
            lent(1, b, r).wait_recv()
            theirs = drecv[1, rows(r), of(lax.rem(b, held), span)]
            total = nbuf[1, rows(r), of(b, span)].astype(F32) + theirs.astype(F32)
            nbuf[1, rows(r), of(b, span)] = total.astype(BF16)
            sends(b, r).start()

        pl.when(inside(spot, b // held == core))(run)

    @scoped
    def down(late, r):
        for j, spot in units[late]:
            landed(j, spot)
            guarded(inside(spot), functools.partial(term, 1, j, spot, r))
        for j, spot in units[late]:
            settle(j, spot, r)

    @scoped
    def down_own(late):
        for j, spot in units[late]:
            landed(j, spot)
            guarded(inside(spot), lambda: each(functools.partial(term, 0, j, spot)))

    def close(j, spot):
        b = where(j, spot)
        local = of(lax.rem(b, held), span)

        def act(r):
            lent(0, b, r).wait_recv()
            sends(b, r).wait_recv()
            ffn = nbuf[0, rows(r), of(b, span)].astype(F32)
            ffn = ffn + drecv[0, rows(r), local].astype(F32)
            ffn = ffn + frecv[rows(r), local].astype(F32)
            after = both[0, rows(r), of(b, span)].astype(F32)
            out[rows(r), local] = (after + ffn).astype(BF16)

        pl.when(inside(spot, b // held == core))(lambda: each(act))

    @scoped
    def end():
        for j, spot in units[0] + units[1]:
            close(j, spot)

    @scoped
    def seq_start():
        for copy in seq_beside:
            copy.start()

    def m_cross_start():
        m_ready()
        for copy in m_cross:
            copy.start()

    @scoped
    def m_wait():
        for copy in m_landed:
            copy.wait_recv()

    def d_cross_start():
        d_ready()
        d_cross.start()

    @scoped
    def d_wait():
        d_landed.wait_recv()

    @scoped
    def pass_seq(r):
        seq_beside[r].wait_recv()
        seq_pass[r].start()

    @scoped
    def seq_wait():
        for copy in seq_pass:
            copy.wait()

    def norm_of(s):
        if s == 0:
            seq_local.wait()
            seq_peer.wait_recv()
        norm(both.at[s], s, 0, length, mix_gain)

    acts = {
        LAUNCH: launch,
        RELAY: relay,
        FINISH: finish,
        ROWS_SWAP: seq_start,
        MIX_SWAP: m_cross_start,
        MIX_WAIT: m_wait,
        DOWN_SWAP: d_cross_start,
        DOWN_WAIT: d_wait,
        ROWS_PASS: pass_seq,
        ROWS_WAIT: seq_wait,
        NORM: norm_of,
        PROJECT: project,
        SCALES: scales,
        MIX_AWAY: functools.partial(mix_terms, 1),
        MIX_OWN: functools.partial(mix_terms, 0),
        MIX_SEND: mix_cross,
        MIX_AFTER: mix_after,
        AFTER_PASS: pass_on,
        FEED_UP: feed_up,
        FEED_GATE: feed,
        DOWN_NEAR: functools.partial(down, 0),
        DOWN_FAR: functools.partial(down, 1),
        DOWN_OWN: down_own,
        END: end,
    }
    seq_peer.start()
    seq_local.start()
    p_ready()
    g_done = False
    for number, (name, *given) in enumerate(ORDER):
        if name == LAUNCH:
            if given[0] in (4, 5) and not g_done:
                g_done = True
                g_ready()
            if full[0] < 4:
                if any(o[:2] == (LAUNCH, given[0]) for o in ORDER[:number]):
                    continue
                given = given[:1]
        if name == RELAY and given[1] >= len(forks[given[0]]):
            continue
        acts[name](*given)
        if name == RELAY and all(o[:2] != (RELAY, given[0]) for o in ORDER[number + 1 :]):
            known = {o[2] for o in ORDER if o[:2] == (RELAY, given[0])}
            for fork in range(len(forks[given[0]])):
                if fork not in known:
                    relay(given[0], fork)
    for part, number, holds in sent:
        guarded(holds, copy_of(part, number).wait_send)
    seq_peer.wait_send()
    d_cross.wait_send()
    for copy in seq_beside + m_cross:
        copy.wait_send()

    def drain(r):
        crossing(r).wait_send()
        for s in range(2):
            exchange(s, r).wait_send()
        spread(r).wait_send()
        afar(r).wait_send()
        onward(r).wait_send()
        for k in range(held):
            sends(core * held + k, r).wait_send()
            for s in range(2):
                lent(s, (1 - core) * held + k, r).wait_send()

    each(drain)


def prepare(full, xp, yp, proj_scales, taps, mix_out_scale, down_scale, ffn_scales, kch, units):
    half = full[0] * full[1] * full[2] // 2
    lines, columns = half // full[2], full[2]
    cols = mix_out_scale.shape[0]
    wide = half * kch
    thin = []
    for scale in (mix_out_scale, down_scale):
        high = lax.reduce_precision(scale, 8, 7)
        middle = lax.reduce_precision(scale - high, 8, 7)
        thin += [high, middle, scale - high - middle]
    thin = jnp.stack(thin)
    ours = (lax.iota(jnp.int32, 2 * cols) // cols == xp)[None]
    thin = jnp.where(ours, jnp.concatenate([thin, thin], 1), 0.0).astype(BF16)
    thin = jnp.pad(thin, ((0, 10), (0, 2 * wide - 2 * cols)))
    chan = jnp.concatenate([proj_scales, taps]).reshape(6, half, 2, 2, kch)
    chan = lax.dynamic_index_in_dim(chan, xp, 2, keepdims=False)
    chan = chan.transpose(2, 0, 1, 3).reshape(2, 6, wide)
    chan = jnp.pad(chan, ((0, 0), (0, 2), (0, 0)))
    hid = ffn_scales.reshape(2, lines, 2, columns, units)
    hid = lax.dynamic_index_in_dim(hid, yp, 2, keepdims=False)
    hid = jnp.pad(hid, ((0, 6), (0, 0), (0, 0), (0, -units % 16))).reshape(8, -1)
    return thin, chan, hid


def body(
    n,
    sequence,
    mix_gain,
    ffn_gain,
    proj_outer,
    proj_inner,
    proj_value,
    proj_scales,
    taps,
    mix_out,
    mix_out_scale,
    ffn_gate,
    ffn_up,
    ffn_scales,
    ffn_down,
    down_scale,
):
    seq = sequence[0]
    length, width = seq.shape
    depth = 2 * width
    full = grid_of(n)
    me = lax.axis_index("fs")
    xp, yp = lax.rem(me, 2), lax.rem(me // full[2], 2)
    kch, units_in = proj_outer.shape[1] // 2, ffn_gate.shape[1]
    thin, chan, hid = prepare(
        full, xp, yp, proj_scales, taps, mix_out_scale, down_scale, ffn_scales, kch, units_in
    )
    members = n // 2
    fch = units_in + -units_in % 16
    cols = mix_out.shape[1]
    ours = 2 * kch * members
    chunks = length // ROWS
    units = members * fch
    dims = [tuple(d // 2 if k == h else d for k, d in enumerate(full)) for h in (X, Y)]
    items = sum(len(routes(dims[g], order)) for g, order in ORDERS)
    held = full[0] * (full[1] // 2)
    operands = (
        seq,
        proj_outer.T,
        proj_inner.T,
        proj_value.T,
        mix_out,
        ffn_gate.T,
        ffn_up.T,
        ffn_down,
        thin,
        chan,
        mix_gain[None],
        ffn_gain[None],
        hid,
    )
    sems = [pltpu.SemaphoreType.DMA((items,))]
    sems += [pltpu.SemaphoreType.DMA((len(ORDERS), members)), pltpu.SemaphoreType.DMA((1,))]
    for k in (4 + 2 * chunks, 2 * chunks, 4 * chunks, 2 * held * chunks, held * chunks):
        sems += [pltpu.SemaphoreType.DMA((k,))] * 2
    result = pl.pallas_call(
        functools.partial(layer_kernel, full),
        out_shape=jax.ShapeDtypeStruct(seq.shape, BF16),
        in_specs=[pl.BlockSpec(memory_space=pltpu.VMEM)] * len(operands),
        out_specs=pl.BlockSpec(memory_space=pltpu.VMEM),
        scratch_shapes=[
            pltpu.VMEM((2, 3, members * kch, depth), BF16),
            pltpu.VMEM((members, 2 * cols + 32, ours), BF16),
            pltpu.VMEM((2, units, depth), BF16),
            pltpu.VMEM((2, members * cols, units), BF16),
            pltpu.VMEM((2, length, depth), BF16),
            pltpu.VMEM((length, depth), BF16),
            pltpu.VMEM((2, length, depth), BF16),
            pltpu.VMEM((2, length, ours), BF16),
            pltpu.VMEM((8 + ROWS, members * kch), F32),
            pltpu.VMEM((2, length, units), BF16),
            pltpu.VMEM((8, depth), F32),
            pltpu.VMEM((cols, ours), BF16),
            pltpu.VMEM((cols, units), BF16),
            pltpu.VMEM((ours, cols), F32),
            pltpu.VMEM((units, cols), F32),
            pltpu.VMEM((2, length, width), BF16),
            pltpu.VMEM((2, length, width), BF16),
            pltpu.VMEM((2, length, width), BF16),
            pltpu.VMEM((length, width), BF16),
            pltpu.VMEM((length, width), BF16),
        ]
        + sems,
        compiler_params=pltpu.CompilerParams(
            collective_id=0, has_side_effects=True, vmem_limit_bytes=67043328
        ),
        name="layer",
    )(*operands)
    return result[None]


def solution(mesh):
    in_specs = (
        P(("rep", "fs"), None, "tp"),
        P(),
        P(),
        P(None, ("tp", "fs")),
        P(None, ("tp", "fs")),
        P(None, ("tp", "fs")),
        P(None, "tp"),
        P(None, "tp"),
        P("tp", "fs"),
        P("fs"),
        P(None, ("tp", "fs")),
        P(None, ("tp", "fs")),
        P(None, "tp"),
        P("tp", "fs"),
        P("fs"),
    )
    out_specs = P(("rep", "fs"), None, "tp")
    return jax.shard_map(
        functools.partial(body, mesh.shape["fs"]),
        mesh=mesh,
        in_specs=in_specs,
        out_specs=out_specs,
        check_vma=False,
    )
```

```python
import functools
import math

import jax
import jax.numpy as jnp
from jax import lax
from jax.experimental import pallas as pl
from jax.experimental.pallas import tpu as pltpu
from jax.sharding import PartitionSpec as P

eps = 1e-06
MESH = pl.DeviceIdType.MESH
BF16 = jnp.bfloat16
F32 = jnp.float32
Z, Y, X = 0, 1, 2
ROWS = 256


def grid_of(n):
    side = 2 ** round(math.log2(n) / 3) if n > 1 else 1
    if n % (side * side):
        side = 1
    return (n // (side * side), side, side)


def routes(dims, order):
    found = []
    frontier = [((0, 0, 0), None, 0, 0)]
    while frontier:
        offset, last, way, depth = frontier.pop(0)
        for place, axis in enumerate(order):
            down = 0 if dims[axis] == 2 else dims[axis] - 1
            for step, limit in ((1, dims[axis] - 1), (-1, down)):
                if last is not None and place < last:
                    continue
                if last == place and step != way:
                    continue
                if abs(offset[axis] + step) > limit:
                    continue
                child = list(offset)
                child[axis] += step
                child = tuple(child)
                found.append((child, offset, axis, step, depth + 1))
                frontier.append((child, place, step, depth + 1))
    return found


def product(rows, columns):
    return lax.dot_general(
        rows, columns, (((1,), (1,)), ((), ())), preferred_element_type=F32
    )


def scoped(act):
    def run(*given):
        numbers = [str(g) for g in given if isinstance(g, int)]
        with jax.named_scope("_".join([act.__name__] + numbers)):
            return act(*given)

    return run


class Group:
    def __init__(self, full, halved, place):
        self.full, self.halved = full, halved
        self.dims = tuple(d // 2 if k == halved else d for k, d in enumerate(full))
        self.place = tuple(p // 2 if k == halved else p for k, p in enumerate(place))
        self.parity = lax.rem(place[halved], 2)
        self.size = self.dims[0] * self.dims[1] * self.dims[2]

    def at(self, offset):
        return [
            lax.rem(self.place[k] + offset[k] + self.dims[k], self.dims[k]) for k in range(3)
        ]

    def index(self, offset):
        at = self.at(offset)
        return (at[0] * self.dims[1] + at[1]) * self.dims[2] + at[2]

    def device(self, offset):
        at = self.at(offset)
        at[self.halved] = 2 * at[self.halved] + self.parity
        return (at[0] * self.full[1] + at[1]) * self.full[2] + at[2]

    def neighbour(self, axis, step):
        return self.device(tuple(step if k == axis else 0 for k in range(3)))

    def slot(self, offset):
        at = [offset[k] % self.dims[k] for k in range(3)]
        return (at[0] * self.dims[1] + at[1]) * self.dims[2] + at[2]

    def within(self, pairs):
        holds = None
        for axis, step in sorted(set(pairs)):
            if self.dims[axis] == 2 or step == 0:
                continue
            at = self.place[axis] + step
            one = (at >= 0) if step < 0 else (at < self.dims[axis])
            holds = one if holds is None else jnp.logical_and(holds, one)
        return holds

    def near(self):
        found = [(axis, 1) for axis in range(3) if self.dims[axis] > 1]
        return found + [(axis, -1) for axis in range(3) if self.dims[axis] > 2]


def guarded(holds, act):
    if holds is None:
        act()
    else:
        pl.when(holds)(act)


def of(step, size):
    if isinstance(step, int):
        return pl.ds(step * size, size)
    return pl.ds(pl.multiple_of(step * size, size), size)


def rows(r):
    return of(r, ROWS)


def to(where, src, dst, send, recv):
    return pltpu.make_async_remote_copy(
        src_ref=src,
        dst_ref=dst,
        send_sem=send,
        recv_sem=recv,
        device_id=where,
        device_id_type=MESH,
    )


ORDERS = [
    (0, (Z, X, Y)),
    (0, (Z, X, Y)),
    (0, (Z, X, Y)),
    (0, (Z, X, Y)),
    (1, (Z, Y, X)),
    (1, (Z, Y, X)),
    (1, (X, Y, Z)),
    (1, (X, Y, Z)),
]
(
    LAUNCH, RELAY, FINISH, ROWS_SWAP, MIX_SWAP, MIX_WAIT, DOWN_SWAP, DOWN_WAIT, ROWS_PASS,
    ROWS_WAIT, NORM, PROJECT, SCALES, MIX_AWAY, MIX_OWN, MIX_SEND, MIX_AFTER, AFTER_PASS, FEED_UP,
    FEED_GATE, DOWN_NEAR, DOWN_FAR, DOWN_OWN, END,
) = range(24)

ORDER = (
    (LAUNCH, 1, 0), (LAUNCH, 1, 1), (MIX_SWAP,), (MIX_WAIT,), (ROWS_SWAP,), (DOWN_SWAP,),
    (LAUNCH, 5, 2), (LAUNCH, 3, 0), (RELAY, 1, 0), (RELAY, 1, 1), (RELAY, 3, 0), (RELAY, 3, 1),
    (DOWN_WAIT,), (LAUNCH, 7, 2), (LAUNCH, 6, 2), (LAUNCH, 2, 0), (LAUNCH, 3, 1), (RELAY, 3, 2),
    (RELAY, 1, 2), (RELAY, 3, 4), (RELAY, 3, 3), (RELAY, 1, 3), (RELAY, 3, 5), (LAUNCH, 0, 0), (LAUNCH, 4, 2),
    (LAUNCH, 5, 0), (LAUNCH, 0, 1), (RELAY, 1, 5), (ROWS_PASS, 0), (RELAY, 0, 1), (LAUNCH, 2, 1),
    (ROWS_PASS, 1), (RELAY, 0, 0), (RELAY, 1, 4), (FINISH, 3), (RELAY, 0, 2), (ROWS_PASS, 2),
    (RELAY, 0, 4), (FINISH, 1), (RELAY, 2, 0), (ROWS_WAIT,), (NORM, 1), (PROJECT, 1, 1), (RELAY, 2, 2),
    (RELAY, 5, 0), (RELAY, 2, 1), (RELAY, 0, 3), (RELAY, 5, 1), (NORM, 0), (RELAY, 0, 5), (RELAY, 2, 4),
    (RELAY, 2, 3), (LAUNCH, 4, 0), (RELAY, 5, 2), (RELAY, 2, 5), (RELAY, 6, 0), (RELAY, 5, 3), (RELAY, 4, 0),
    (LAUNCH, 6, 0), (RELAY, 4, 1), (FINISH, 0), (PROJECT, 0, 1), (FINISH, 2), (SCALES,), (MIX_AWAY, 0),
    (MIX_AWAY, 1), (LAUNCH, 7, 0), (MIX_AWAY, 2), (MIX_SEND, 0), (MIX_SEND, 1), (MIX_SEND, 2),
    (RELAY, 5, 5), (RELAY, 6, 4), (PROJECT, 1, 0), (RELAY, 7, 0), (PROJECT, 0, 0), (RELAY, 5, 4),
    (MIX_OWN, 0), (MIX_AFTER, 0), (RELAY, 4, 3), (MIX_OWN, 1), (MIX_AFTER, 1), (RELAY, 4, 2),
    (RELAY, 7, 3), (RELAY, 6, 2), (AFTER_PASS, 0), (RELAY, 4, 4), (FINISH, 5), (RELAY, 7, 2), (RELAY, 6, 8),
    (FEED_UP, 1, 0), (MIX_OWN, 2), (RELAY, 6, 6), (FEED_UP, 0, 1), (MIX_AFTER, 2), (AFTER_PASS, 1),
    (RELAY, 4, 5), (RELAY, 6, 3), (RELAY, 7, 7), (FEED_UP, 1, 1), (RELAY, 7, 4), (RELAY, 7, 1), (RELAY, 6, 7),
    (RELAY, 6, 1), (FINISH, 4), (FEED_GATE, 1, 0), (DOWN_NEAR, 0), (AFTER_PASS, 2), (FEED_GATE, 1, 1),
    (DOWN_NEAR, 1), (FEED_UP, 1, 2), (FEED_GATE, 1, 2), (DOWN_NEAR, 2), (RELAY, 7, 8), (RELAY, 7, 6),
    (RELAY, 7, 5), (RELAY, 6, 5), (DOWN_FAR, 0), (DOWN_FAR, 1), (FEED_UP, 0, 2), (FEED_UP, 0, 0),
    (DOWN_FAR, 2), (FEED_GATE, 0, 0), (FEED_GATE, 0, 1), (FEED_GATE, 0, 2), (DOWN_OWN, 0), (DOWN_OWN, 1),
    (END,),
)


def layer_kernel(
    full,
    seq,
    po_in,
    pi_in,
    pv_in,
    m_in,
    gate_in,
    up_in,
    d_in,
    thin,
    chan,
    mix_gain,
    ffn_gain,
    hid,
    out,
    pbuf,
    mbuf,
    gbuf,
    dbuf,
    both,
    aft,
    nbuf,
    gated,
    ext,
    hbuf,
    sbuf,
    m_out,
    d_out,
    m_tmp,
    d_tmp,
    dsend,
    drecv,
    xsend,
    xrecv,
    frecv,
    w_send,
    w_recv,
    own_sem,
    s_send,
    s_recv,
    x_send,
    x_recv,
    c_send,
    c_recv,
    d_send,
    d_recv,
    y_send,
    y_recv,
):
    me = lax.axis_index("fs")
    core = lax.axis_index("tp")
    peer = {"tp": 1 - core}
    here = (me // (full[1] * full[2]), lax.rem(me // full[2], full[1]), lax.rem(me, full[2]))
    mixer, feeder = Group(full, X, here), Group(full, Y, here)
    groups = (mixer, feeder)
    xp, yp = mixer.parity, feeder.parity
    beside = {"fs": me + 1 - 2 * xp}
    across = {"fs": me + (1 - 2 * yp) * full[2]}
    members = mixer.size
    length, width = seq.shape
    chunks = length // ROWS
    kch = po_in.shape[0] // 2
    units_in = gate_in.shape[0]
    units_sent = units_in + -units_in % 8
    fch = gbuf.shape[1] // members
    cols = m_in.shape[1]
    pair = 2 * cols
    span = full[2] * cols
    wide = kch * members
    hidden = fch * members
    origin = (0, 0, 0)
    cut = (pair + 32) // 2 // 16 * 16
    views = [
        lambda i: pbuf.at[0, :, of(i, kch)],
        lambda i: pbuf.at[1, :, of(i, kch)],
        lambda i: mbuf.at[i, pl.ds(0, cut)],
        lambda i: mbuf.at[i, pl.ds(cut, pair + 32 - cut)],
        lambda i: gbuf.at[0, pl.ds(pl.multiple_of(i * fch, 16), units_sent)],
        lambda i: gbuf.at[1, pl.ds(pl.multiple_of(i * fch, 16), units_sent)],
        lambda i: dbuf.at[0, of(i, cols)],
        lambda i: dbuf.at[1, of(i, cols)],
    ]
    plans = [routes(groups[g].dims, order) for g, order in ORDERS]
    base = [sum(len(p) for p in plans[:k]) for k in range(len(plans))]
    deepest = [max(item[4] for item in p) for p in plans]
    arrived = [set() for _ in plans]
    sent = []

    def copy_of(part, number):
        group = groups[ORDERS[part][0]]
        child, parent, axis, step, _ = plans[part][number]
        home = views[part](group.index(parent))
        return to(
            {"fs": group.neighbour(axis, -step)},
            home,
            home,
            w_send.at[base[part] + number],
            w_recv.at[part, group.slot(child)],
        )

    def launch(part, only=None, parent=origin):
        group = groups[ORDERS[part][0]]
        for number, item in enumerate(plans[part]):
            if item[1] == parent and only in (None, item[2]):
                holds = group.within(list(enumerate(parent)) + [(item[2], -item[3])])
                guarded(holds, copy_of(part, number).start)
                sent.append((part, number, holds))

    def arrive(part, child):
        if child in arrived[part] or child == origin:
            return
        arrived[part].add(child)
        group = groups[ORDERS[part][0]]
        block = views[part](group.index(child))
        there = to(
            peer, block, block, w_send.at[0], w_recv.at[part, group.slot(child)]
        )
        guarded(group.within(list(enumerate(child))), there.wait_recv)

    forks = []
    for plan in plans:
        found = []
        for item in sorted(plan, key=lambda item: item[4]):
            if item[1] != origin and item[1] not in found:
                found.append(item[1])
        forks.append(found)

    @scoped
    def relay(part, number):
        arrive(part, forks[part][number])
        launch(part, None, forks[part][number])

    @scoped
    def finish(part):
        for item in plans[part]:
            arrive(part, item[0])

    if fch > units_in:
        for which in range(2):
            for i in range(members):
                spot = pl.ds(i * fch + units_in, fch - units_in)
                gbuf[which, spot, :] = jnp.zeros((fch - units_in, 2 * width), BF16)

    barrier = pltpu.get_barrier_semaphore()
    greeted = [{"fs": g.neighbour(*hop)} for g in groups for hop in g.near()]
    greeted += [beside, across, peer]
    for device in greeted:
        pl.semaphore_signal(barrier, inc=1, device_id=device, device_id_type=MESH)
    pl.semaphore_wait(barrier, len(greeted))

    mine = of(core, width)

    seq_local = pltpu.make_async_copy(seq, both.at[0, :, mine], own_sem.at[0])
    seq_peer = to(peer, seq, both.at[0, :, mine], s_send.at[0], s_recv.at[0])
    seq_beside, seq_pass = [], []
    for r in range(chunks):
        home = both.at[1, rows(r), mine]
        seq_beside.append(
            to(beside, seq.at[rows(r)], home, s_send.at[1 + r], s_recv.at[1 + r])
        )
        at = 1 + chunks + r
        seq_pass.append(to(peer, home, home, s_send.at[at], s_recv.at[at]))
    side = of(xp, cols)
    ends = pl.ds(pl.multiple_of(pair + xp * 16, 16), 16)
    at = 1 + 2 * chunks
    m_home = mbuf.at[mixer.index(origin), side]
    e_home = mbuf.at[mixer.index(origin), ends]
    d_home = dbuf.at[yp, of(feeder.index(origin), cols)]
    m_cross = [
        to(beside, m_out, m_home, s_send.at[at], s_recv.at[at]),
        to(beside, thin, e_home, s_send.at[at + 1], s_recv.at[at + 1]),
    ]
    d_cross = to(across, d_out, d_home, s_send.at[at + 2], s_recv.at[at + 2])
    d_there = dbuf.at[1 - yp, of(feeder.index(origin), cols)]
    d_landed = to(across, d_there, d_there, s_send.at[at + 2], s_recv.at[at + 2])
    m_there = [
        mbuf.at[mixer.index(origin), of(1 - xp, cols)],
        mbuf.at[
            mixer.index(origin), pl.ds(pl.multiple_of(pair + (1 - xp) * 16, 16), 16)
        ],
    ]
    m_landed = [
        to(beside, ref, ref, s_send.at[at + k], s_recv.at[at + k])
        for k, ref in enumerate(m_there)
    ]

    @scoped
    def p_ready():
        spot = of(mixer.index(origin), kch)
        for k in range(2):
            for which, ref in enumerate((po_in, pi_in, pv_in)):
                pbuf[k, which, spot, :] = ref[pl.ds(k * kch, kch), :].astype(BF16)

    @scoped
    def g_ready():
        spot = pl.ds(pl.multiple_of(feeder.index(origin) * fch, 16), units_in)
        for which, ref in enumerate((gate_in, up_in)):
            gbuf[which, spot, :] = ref[...].astype(BF16)

    @scoped
    def m_ready():
        each_in = 2 * kch
        for target in range(2):
            to_x = xp if target else 1 - xp
            for g in range(members):
                for k in range(2):
                    source = pl.multiple_of((2 * g + to_x) * each_in + k * kch, kch)
                    m_tmp[pl.ds(k * wide + g * kch, kch), :] = m_in[pl.ds(source, kch), :]
            for tile in range(m_tmp.shape[0] // 128):
                at_ = pl.ds(tile * 128, 128)
                turned = m_tmp[at_, :].T.astype(BF16)
                if target:
                    m_home[:, at_] = turned
                else:
                    m_out[:, at_] = turned
        e_home[...] = thin[...]

    @scoped
    def d_ready():
        for target in range(2):
            to_y = yp if target else 1 - yp
            for i in range(members):
                line, x = i // full[2], i % full[2]
                source = ((2 * line + to_y) * full[2] + x) * units_in
                spot = pl.ds(i * fch, units_in)
                d_tmp[spot, :] = d_in[pl.ds(pl.multiple_of(source, 4), units_in), :]
                if fch > units_in:
                    fill = fch - units_in
                    d_tmp[pl.ds(i * fch + units_in, fill), :] = jnp.zeros((fill, cols), F32)
            for tile in range(d_tmp.shape[0] // 128):
                at_ = pl.ds(tile * 128, 128)
                turned = d_tmp[at_, :].T.astype(BF16)
                if target:
                    d_home[:, at_] = turned
                else:
                    d_out[:, at_] = turned

    @scoped
    def norm(source, target, first, count, gains):
        tall, deep = 16, 4

        def step(i, _):
            spots = [
                pl.ds(pl.multiple_of(first + (i * deep + k) * tall, tall), tall)
                for k in range(deep)
            ]
            factors = []
            for spot in spots:
                values = source[spot, :].astype(F32)
                mean = jnp.mean(values * values, axis=-1, keepdims=True)
                factors.append(lax.rsqrt(mean + eps))
            for spot, factor in zip(spots, factors):
                scaled = source[spot, :].astype(F32) * factor
                nbuf[target, spot, :] = (scaled * gains[...]).astype(BF16)
            return 0

        lax.fori_loop(0, count // (tall * deep), step, 0)

    def each(act):
        def step(r, _):
            act(r)
            return 0

        lax.fori_loop(0, chunks, step, 0)

    @scoped
    def project(k, s):
        ext[0:8, :] = jnp.zeros((8, wide), F32)

        def act(r):
            block = nbuf[s, rows(r), :]
            inner = product(block, pbuf[k, 1]) * chan[k, 1:2, :]
            value = product(block, pbuf[k, 2]) * chan[k, 2:3, :]
            carried = inner * value
            ext[8 : 8 + ROWS, :] = carried
            conv = chan[k, 3:4, :] * ext[6 : 6 + ROWS, :]
            conv = conv + chan[k, 4:5, :] * ext[7 : 7 + ROWS, :]
            conv = conv + chan[k, 5:6, :] * carried
            ext[0:8, :] = ext[ROWS : ROWS + 8, :]
            outer = product(block, pbuf[k, 0]) * chan[k, 0:1, :]
            gated[s, rows(r), pl.ds(k * wide, wide)] = (outer * conv).astype(BF16)

        each(act)

    @scoped
    def scales():
        def step(g, _):
            tiles = [
                mbuf[g, pl.ds(pair + 16 * e, 16), pl.ds(0, pair)].astype(F32)
                for e in range(2)
            ]
            for which in range(2):
                scale = jnp.zeros((1, pair), F32)
                for tile in tiles:
                    for k in range(3):
                        scale = scale + tile[3 * which + k : 3 * which + k + 1]
                sbuf[which : which + 1, of(g, pair)] = scale
            return 0

        lax.fori_loop(0, members, step, 0)

    def exchange(s, r):
        at = s * chunks + r
        home = drecv.at[s, rows(r)]
        return to(peer, dsend.at[s, rows(r)], home, c_send.at[at], c_recv.at[at])

    def crossing(r):
        return to(beside, xsend.at[1, rows(r)], xrecv.at[rows(r)], x_send.at[r], x_recv.at[r])

    def spread(r):
        at = 2 * chunks + r
        home = both.at[0, rows(r), mine]
        return to(peer, home, home, c_send.at[at], c_recv.at[at])

    def afar(r):
        at = chunks + r
        return to(
            across, both.at[0, rows(r), mine], aft.at[rows(r), mine], x_send.at[at], x_recv.at[at]
        )

    def onward(r):
        at = 3 * chunks + r
        home = aft.at[rows(r), mine]
        return to(peer, home, home, c_send.at[at], c_recv.at[at])

    half = members // 2

    @scoped
    def mix_terms(s, r):
        def block(g, ref, i):
            term = product(gated[s, rows(r), :], mbuf[g, pl.ds(0, pair), :])
            ref[s, rows(r), of(i, pair)] = (term * sbuf[0:1, of(g, pair)]).astype(BF16)

        for i in range(half):
            block((1 - core) * half + i, dsend, i)
        exchange(s, r).start()
        for i in range(half):
            block(core * half + i, xsend, i)

    @scoped
    def mix_cross(r):
        exchange(1, r).wait_recv()
        total = xsend[1, rows(r), :].astype(F32) + drecv[1, rows(r), :].astype(F32)
        xsend[1, rows(r), :] = total.astype(BF16)
        crossing(r).start()

    @scoped
    def mix_after(r):
        exchange(0, r).wait_recv()
        crossing(r).wait_recv()
        mix = xsend[0, rows(r), :].astype(F32) + drecv[0, rows(r), :].astype(F32)
        mix = mix + xrecv[rows(r), :].astype(F32)
        after = both[0, rows(r), mine].astype(F32) + mix
        both[0, rows(r), mine] = after.astype(BF16)
        afar(r).start()
        spread(r).start()

    @scoped
    def pass_on(r):
        afar(r).wait_recv()
        onward(r).start()

    def wide_steps(act):
        def step(i, _):
            act(of(i, wide))
            return 0

        lax.fori_loop(0, hidden // wide, step, 0)

    @scoped
    def feed_up(s, r):
        (spread, onward)[s](r).wait_recv()
        norm((both.at[0], aft)[s], s, r * ROWS, ROWS, ffn_gain)

        def act(at):
            up = product(nbuf[s, rows(r), :], gbuf[1, at, :]) * hid[1:2, at]
            hbuf[s, rows(r), at] = up.astype(BF16)

        wide_steps(act)

    @scoped
    def feed(s, r):
        def act(at):
            gate = product(nbuf[s, rows(r), :], gbuf[0, at, :]) * hid[0:1, at]
            up = hbuf[s, rows(r), at].astype(F32)
            hbuf[s, rows(r), at] = (gate / (1.0 + jnp.exp(-gate)) * up).astype(BF16)

        wide_steps(act)

    blocks = 2 * feeder.dims[0] * feeder.dims[1]
    held = blocks // 2

    def where(j, spot):
        at = feeder.at(spot)
        return (at[0] * feeder.dims[1] + at[1]) * 2 + j

    def inside(spot, holds=None):
        there = feeder.within(list(enumerate(spot)))
        if there is None or holds is None:
            return holds if there is None else there
        return jnp.logical_and(holds, there)

    def lent(s, b, r):
        at = (s * held + lax.rem(b, held)) * chunks + r
        local = of(lax.rem(b, held), span)
        return to(
            peer,
            nbuf.at[s, rows(r), of(b, span)],
            drecv.at[s, rows(r), local],
            d_send.at[at],
            d_recv.at[at],
        )

    def sends(b, r):
        at = lax.rem(b, held) * chunks + r
        local = of(lax.rem(b, held), span)
        return to(
            across,
            nbuf.at[1, rows(r), of(b, span)],
            frecv.at[rows(r), local],
            y_send.at[at],
            y_recv.at[at],
        )

    spots = sorted(
        {(item[0][0], item[0][1], 0) for item in plans[6]} | {origin},
        key=lambda o: (abs(o[0]) + abs(o[1]), o),
    )
    units = [
        [(j, spot) for spot in spots for j in range(2) if (abs(spot[0]) + abs(spot[1]) < 2) == near]
        for near in (True, False)
    ]

    def landed(j, spot):
        for item in plans[6 + j]:
            if item[0][:2] == spot[:2]:
                arrive(6 + j, item[0])

    def term(s, j, spot, r):
        b = where(j, spot)
        value = product(hbuf[s, rows(r), :], dbuf[j, of(b // 2, span), :])
        value = value * sbuf[1:2, of(b, span)]
        nbuf[s, rows(r), of(b, span)] = value.astype(BF16)
        pl.when(b // held != core)(lent(s, b, r).start)

    def settle(j, spot, r):
        b = where(j, spot)

        def run():
            lent(1, b, r).wait_recv()
            theirs = drecv[1, rows(r), of(lax.rem(b, held), span)]
            total = nbuf[1, rows(r), of(b, span)].astype(F32) + theirs.astype(F32)
            nbuf[1, rows(r), of(b, span)] = total.astype(BF16)
            sends(b, r).start()

        pl.when(inside(spot, b // held == core))(run)

    @scoped
    def down(late, r):
        for j, spot in units[late]:
            landed(j, spot)
            guarded(inside(spot), functools.partial(term, 1, j, spot, r))
        for j, spot in units[late]:
            settle(j, spot, r)

    @scoped
    def down_own(late):
        for j, spot in units[late]:
            landed(j, spot)
            guarded(inside(spot), lambda: each(functools.partial(term, 0, j, spot)))

    def close(j, spot):
        b = where(j, spot)
        local = of(lax.rem(b, held), span)

        def act(r):
            lent(0, b, r).wait_recv()
            sends(b, r).wait_recv()
            ffn = nbuf[0, rows(r), of(b, span)].astype(F32)
            ffn = ffn + drecv[0, rows(r), local].astype(F32)
            ffn = ffn + frecv[rows(r), local].astype(F32)
            after = both[0, rows(r), of(b, span)].astype(F32)
            out[rows(r), local] = (after + ffn).astype(BF16)

        pl.when(inside(spot, b // held == core))(lambda: each(act))

    @scoped
    def end():
        for j, spot in units[0] + units[1]:
            close(j, spot)

    @scoped
    def seq_start():
        for copy in seq_beside:
            copy.start()

    def m_cross_start():
        m_ready()
        for copy in m_cross:
            copy.start()

    @scoped
    def m_wait():
        for copy in m_landed:
            copy.wait_recv()

    def d_cross_start():
        d_ready()
        d_cross.start()

    @scoped
    def d_wait():
        d_landed.wait_recv()

    @scoped
    def pass_seq(r):
        seq_beside[r].wait_recv()
        seq_pass[r].start()

    @scoped
    def seq_wait():
        for copy in seq_pass:
            copy.wait()

    def norm_of(s):
        if s == 0:
            seq_local.wait()
            seq_peer.wait_recv()
        norm(both.at[s], s, 0, length, mix_gain)

    acts = {
        LAUNCH: launch,
        RELAY: relay,
        FINISH: finish,
        ROWS_SWAP: seq_start,
        MIX_SWAP: m_cross_start,
        MIX_WAIT: m_wait,
        DOWN_SWAP: d_cross_start,
        DOWN_WAIT: d_wait,
        ROWS_PASS: pass_seq,
        ROWS_WAIT: seq_wait,
        NORM: norm_of,
        PROJECT: project,
        SCALES: scales,
        MIX_AWAY: functools.partial(mix_terms, 1),
        MIX_OWN: functools.partial(mix_terms, 0),
        MIX_SEND: mix_cross,
        MIX_AFTER: mix_after,
        AFTER_PASS: pass_on,
        FEED_UP: feed_up,
        FEED_GATE: feed,
        DOWN_NEAR: functools.partial(down, 0),
        DOWN_FAR: functools.partial(down, 1),
        DOWN_OWN: down_own,
        END: end,
    }
    seq_peer.start()
    seq_local.start()
    p_ready()
    g_done = False
    for number, (name, *given) in enumerate(ORDER):
        if name == LAUNCH:
            if given[0] in (4, 5) and not g_done:
                g_done = True
                g_ready()
            if full[0] < 4:
                if any(o[:2] == (LAUNCH, given[0]) for o in ORDER[:number]):
                    continue
                given = given[:1]
        if name == RELAY and given[1] >= len(forks[given[0]]):
            continue
        acts[name](*given)
        if name == RELAY and all(o[:2] != (RELAY, given[0]) for o in ORDER[number + 1 :]):
            known = {o[2] for o in ORDER if o[:2] == (RELAY, given[0])}
            for fork in range(len(forks[given[0]])):
                if fork not in known:
                    relay(given[0], fork)
    for part, number, holds in sent:
        guarded(holds, copy_of(part, number).wait_send)
    seq_peer.wait_send()
    d_cross.wait_send()
    for copy in seq_beside + m_cross:
        copy.wait_send()

    def drain(r):
        crossing(r).wait_send()
        for s in range(2):
            exchange(s, r).wait_send()
        spread(r).wait_send()
        afar(r).wait_send()
        onward(r).wait_send()
        for k in range(held):
            sends(core * held + k, r).wait_send()
            for s in range(2):
                lent(s, (1 - core) * held + k, r).wait_send()

    each(drain)


def prepare(full, xp, yp, proj_scales, taps, mix_out_scale, down_scale, ffn_scales, kch, units):
    half = full[0] * full[1] * full[2] // 2
    lines, columns = half // full[2], full[2]
    cols = mix_out_scale.shape[0]
    wide = half * kch
    thin = []
    for scale in (mix_out_scale, down_scale):
        high = lax.reduce_precision(scale, 8, 7)
        middle = lax.reduce_precision(scale - high, 8, 7)
        thin += [high, middle, scale - high - middle]
    thin = jnp.stack(thin)
    ours = (lax.iota(jnp.int32, 2 * cols) // cols == xp)[None]
    thin = jnp.where(ours, jnp.concatenate([thin, thin], 1), 0.0).astype(BF16)
    thin = jnp.pad(thin, ((0, 10), (0, 2 * wide - 2 * cols)))
    chan = jnp.concatenate([proj_scales, taps]).reshape(6, half, 2, 2, kch)
    chan = lax.dynamic_index_in_dim(chan, xp, 2, keepdims=False)
    chan = chan.transpose(2, 0, 1, 3).reshape(2, 6, wide)
    hid = ffn_scales.reshape(2, lines, 2, columns, units)
    hid = lax.dynamic_index_in_dim(hid, yp, 2, keepdims=False)
    hid = jnp.pad(hid, ((0, 0), (0, 0), (0, 0), (0, -units % 16))).reshape(2, -1)
    return thin, chan, hid


def body(
    n,
    sequence,
    mix_gain,
    ffn_gain,
    proj_outer,
    proj_inner,
    proj_value,
    proj_scales,
    taps,
    mix_out,
    mix_out_scale,
    ffn_gate,
    ffn_up,
    ffn_scales,
    ffn_down,
    down_scale,
):
    seq = sequence[0]
    length, width = seq.shape
    depth = 2 * width
    full = grid_of(n)
    me = lax.axis_index("fs")
    xp, yp = lax.rem(me, 2), lax.rem(me // full[2], 2)
    kch, units_in = proj_outer.shape[1] // 2, ffn_gate.shape[1]
    thin, chan, hid = prepare(
        full, xp, yp, proj_scales, taps, mix_out_scale, down_scale, ffn_scales, kch, units_in
    )
    members = n // 2
    fch = units_in + -units_in % 16
    cols = mix_out.shape[1]
    ours = 2 * kch * members
    chunks = length // ROWS
    units = members * fch
    dims = [tuple(d // 2 if k == h else d for k, d in enumerate(full)) for h in (X, Y)]
    items = sum(len(routes(dims[g], order)) for g, order in ORDERS)
    held = full[0] * (full[1] // 2)
    operands = (
        seq,
        proj_outer.T,
        proj_inner.T,
        proj_value.T,
        mix_out,
        ffn_gate.T,
        ffn_up.T,
        ffn_down,
        thin,
        chan,
        mix_gain[None],
        ffn_gain[None],
        hid,
    )
    sems = [pltpu.SemaphoreType.DMA((items,))]
    sems += [pltpu.SemaphoreType.DMA((len(ORDERS), members)), pltpu.SemaphoreType.DMA((1,))]
    for k in (4 + 2 * chunks, 2 * chunks, 4 * chunks, 2 * held * chunks, held * chunks):
        sems += [pltpu.SemaphoreType.DMA((k,))] * 2
    result = pl.pallas_call(
        functools.partial(layer_kernel, full),
        out_shape=jax.ShapeDtypeStruct(seq.shape, BF16),
        in_specs=[pl.BlockSpec(memory_space=pltpu.VMEM)] * len(operands),
        out_specs=pl.BlockSpec(memory_space=pltpu.VMEM),
        scratch_shapes=[
            pltpu.VMEM((2, 3, members * kch, depth), BF16),
            pltpu.VMEM((members, 2 * cols + 32, ours), BF16),
            pltpu.VMEM((2, units, depth), BF16),
            pltpu.VMEM((2, members * cols, units), BF16),
            pltpu.VMEM((2, length, depth), BF16),
            pltpu.VMEM((length, depth), BF16),
            pltpu.VMEM((2, length, depth), BF16),
            pltpu.VMEM((2, length, ours), BF16),
            pltpu.VMEM((8 + ROWS, members * kch), F32),
            pltpu.VMEM((2, length, units), BF16),
            pltpu.VMEM((8, depth), F32),
            pltpu.VMEM((cols, ours), BF16),
            pltpu.VMEM((cols, units), BF16),
            pltpu.VMEM((ours, cols), F32),
            pltpu.VMEM((units, cols), F32),
            pltpu.VMEM((2, length, width), BF16),
            pltpu.VMEM((2, length, width), BF16),
            pltpu.VMEM((2, length, width), BF16),
            pltpu.VMEM((length, width), BF16),
            pltpu.VMEM((length, width), BF16),
        ]
        + sems,
        compiler_params=pltpu.CompilerParams(
            collective_id=0, has_side_effects=True, vmem_limit_bytes=67043328
        ),
        name="layer",
    )(*operands)
    return result[None]


def solution(mesh):
    in_specs = (
        P(("rep", "fs"), None, "tp"),
        P(),
        P(),
        P(None, ("tp", "fs")),
        P(None, ("tp", "fs")),
        P(None, ("tp", "fs")),
        P(None, "tp"),
        P(None, "tp"),
        P("tp", "fs"),
        P("fs"),
        P(None, ("tp", "fs")),
        P(None, ("tp", "fs")),
        P(None, "tp"),
        P("tp", "fs"),
        P("fs"),
    )
    out_specs = P(("rep", "fs"), None, "tp")
    return jax.shard_map(
        functools.partial(body, mesh.shape["fs"]),
        mesh=mesh,
        in_specs=in_specs,
        out_specs=out_specs,
        check_vma=False,
    )
```
